256 devices in a mesh: sp: 64 (over z, y, core), tp: 4 (over x).
Axes of the slice: x: 4, y: 4, z: 8, core: 2. Of those that a mesh axis runs over, the one named last changes fastest.
Arguments:
- glu_value: bfloat16 [32768, 2048], P('sp', 'tp'), may hold values from -640 to 640
- glu_gate: bfloat16 [32768, 2048], P('sp', 'tp'), may hold values from -9 to 9
- conv_kernel: float32 [31, 2048], P(None, 'tp'), may hold values from -1 to 1
- norm_gain: float32 [2048], P('tp'), may hold values from 0.1 to 1.9
- mix_weight: bfloat16 [2048, 2048], P('tp'), may hold values from -0.125 to 0.125
- residual: bfloat16 [32768, 2048], P(('sp', 'tp')), may hold values from -6 to 6
- resid_gain: float32 [2048], replicated, may hold values from 0.1 to 1.9
- expert_ids: int32 [32768, 2], P(('sp', 'tp')), may hold values from 0 to 63, all different within a row; in each aligned block of 128 rows (0 to 127, 128 to 255, ...) at most 8 rows name the same one
- route_weight: float32 [32768, 2], P(('sp', 'tp')), may hold values from 0.05 to 0.5
- w_gate: bfloat16 [64, 2048, 2048], P('sp', None, 'tp'), may hold values from -0.5 to 0.5
- w_up: bfloat16 [64, 2048, 2048], P('sp', None, 'tp'), may hold values from -0.5 to 0.5
- w_down: bfloat16 [64, 2048, 2048], P('sp', 'tp'), may hold values from -0.03125 to 0.03125
- out_gain: float32 [2048], replicated, may hold values from 0.1 to 1.9
Outputs:
- blended: bfloat16 [32768, 2048], P(('sp', 'tp'))
The draws below stay inside these ranges and needn't reach their ends.
Inputs may be any that keep to these rules, and one draw needn't show every extreme that they name: `expert_ids`: in each aligned block of 128 rows (the rows of one device) no expert is named by more than 8 rows, a bound that some block reaches.
All inputs are finite; a program needn't handle non-finite values.
Results may differ from the reference program's by a relative error of at most 0.015.
Values may be sent and summed in bfloat16 or wider, within the bound.
A program may use at most 128 MiB of HBM per device.

```python
import math
from functools import partial
import jax
import jax.numpy as jnp
import numpy as np
from jax import lax

D = 2048
DC = 2048
FFE = 2048
KERNEL = 31
TOPK = 2
TOKENS = 32768
BLOCK = 128
EXPERTS = 64
CAP = 8
N_SP = 64
N_TP = 4


def draw_glu_value(key, part):
    key_rough, key_base = jax.random.split(key, 2)
    ramp = 10.0 ** (jnp.arange(DC, dtype=jnp.float32) / DC)
    rough = jax.random.uniform(key_rough, (DC,), jnp.float32, 0.5, 1.5)
    base = jnp.clip(jax.random.normal(key_base, (TOKENS, DC), jnp.float32), -6.0, 6.0)
    return (0.5 * ramp * rough * base).astype(jnp.bfloat16)


def shard_levels(own_key, extent, cuts, least, high):
    level = 1.0
    for dim, shards_of in cuts:
        steps = jax.random.uniform(jax.random.fold_in(jax.random.fold_in(own_key, 6), dim), (shards_of,), jnp.float32, least / len(cuts), high / len(cuts))
        level = level * jnp.repeat(jnp.exp(steps), extent[dim] // shards_of).reshape((-1,) + (1,) * (len(extent) - 1 - dim))
    return level


def routed_block(rng, own, number, rows, number_of, top, bound, skew):
    order = jax.random.permutation(rng, number_of)
    crowded, usual = portions_of(number_of, rows * top, bound, skew, True), portions_of(number_of, rows * top, bound, skew, False)
    places = jnp.arange(number_of)

    def named(tallies, turn):
        used = int((tallies > 0).sum())
        fixed = max(1, used // 4)
        moved = fixed + (places - fixed + turn * (used - fixed)) % max(1, number_of - fixed)
        return jnp.zeros((number_of,), jnp.int32).at[order[jnp.where(places < fixed, places, moved)]].set(jnp.asarray(tallies, jnp.int32))

    tallies = jnp.where(number % 4 == 0, named(crowded, number // 4), named(usual, number - number // 4 - 1))
    mixed = jax.random.permutation(jax.random.fold_in(own, 3), number_of)
    giver, sink = mixed[0:number_of // 2 * 2:2], mixed[1:number_of // 2 * 2:2]
    margin = jnp.minimum(tallies[giver] - 1, bound - tallies[sink]) // 2
    margin = jnp.where((giver == order[0]) | (sink == order[0]) | (tallies[sink] == 0), 0, jnp.maximum(margin, 0))
    moved = jax.random.randint(jax.random.fold_in(own, 4), (number_of // 2,), 0, 1 << 20) % (margin + 1)
    tallies = tallies.at[giver].add(-moved).at[sink].add(moved)
    items = jnp.searchsorted(jnp.cumsum(tallies), jnp.arange(rows * top), side="right").astype(jnp.int32)
    grid = items.reshape(top, rows).T
    grid = grid[jax.random.permutation(jax.random.fold_in(own, 1), rows)]
    turn = jax.random.randint(jax.random.fold_in(own, 2), (rows, 1), 0, top)
    return jnp.take_along_axis(grid, (jnp.arange(top)[None, :] + turn) % top, axis=1)


def portions_of(number_of, total, reach, skew, full):
    loads = [(1 << 20) // math.isqrt(rank ** skew) + 1 for rank in range(1, number_of + 1)]
    largest = reach if full else min(reach, max(-(-total // number_of), total * loads[0] // sum(loads)))
    least = 1 if total - largest >= number_of - 1 else 0
    holding, spare = [largest] + [least] * (number_of - 1), total - largest - least * (number_of - 1)
    while spare > 0:
        candidates = [i for i in range(1, number_of) if holding[i] < largest] or [i for i in range(1, number_of) if holding[i] < reach]
        mass, budget = sum([loads[i] for i in candidates]), spare
        for i in candidates:
            addition = min(reach - holding[i], max(1, budget * loads[i] // mass), spare)
            holding[i] = holding[i] + addition
            spare = spare - addition
    return np.array(holding)


def noise(stream_key, dims, scale, limit, cuts=(), kind=jnp.bfloat16):
    factor_of = shard_levels(stream_key, dims, cuts, -0.22, 0.18) if cuts else 1.0
    values = jax.random.normal(stream_key, dims, jnp.float32) * scale * factor_of
    return jnp.minimum(jnp.maximum(values, -limit), limit).astype(kind)


def setup_inputs(seed: int = 0) -> dict:
    splits = jax.random.split(jax.random.key(seed), 14)
    glu_value = draw_glu_value(jax.random.fold_in(splits[13], 71), 0)
    glu_gate = noise(splits[1], (TOKENS, DC), 1.5, 9.0, ((0, 64), (1, 4)))
    conv_kernel = noise(splits[2], (KERNEL, DC), KERNEL ** -0.5, 1.0, ((1, 4),), jnp.float32)
    norm_gain = jnp.clip(1.0 + 0.18 * jax.random.normal(splits[3], (DC,), jnp.float32), 0.1, 1.9)
    mix_weight = noise(splits[4], (DC, D), DC ** -0.5, 0.125, ((0, 4),))
    residual = noise(splits[5], (TOKENS, D), 1.0, 6.0, ((0, 256),))
    resid_gain = jnp.clip(1.0 + 0.18 * jax.random.normal(splits[6], (D,), jnp.float32), 0.1, 1.9)
    expert_ids_keys = jax.random.split(jax.random.fold_in(splits[7], 1), TOKENS // BLOCK)
    expert_ids_turns = jax.random.permutation(jax.random.fold_in(splits[7], 3), TOKENS // BLOCK)
    expert_ids = jax.vmap(lambda own, number: routed_block(jax.random.fold_in(splits[7], 2), own, number, BLOCK, EXPERTS, TOPK, CAP, 2))(expert_ids_keys, expert_ids_turns).reshape((TOKENS, TOPK))
    route_weight = jnp.clip(jnp.exp(math.log(0.5) - 2.3025851 * jax.random.uniform(splits[8], (TOKENS, TOPK), jnp.float32) ** shard_levels(splits[8], (TOKENS, TOPK), ((0, 256),), -0.2, 0.2)), 0.05, 0.5)
    w_gate = noise(splits[9], (EXPERTS, D, FFE), (D // 16) ** -0.5, 0.5, ((0, 64), (2, 4)))
    w_up = noise(splits[10], (EXPERTS, D, FFE), (D // 16) ** -0.5, 0.5, ((0, 64), (2, 4)))
    w_down = noise(splits[11], (EXPERTS, FFE, D), (16 * FFE) ** -0.5, 0.03125, ((0, 64), (1, 4)))
    out_gain = jnp.clip(1.0 + 0.18 * jax.random.normal(splits[12], (D,), jnp.float32), 0.1, 1.9)
    return {"glu_value": glu_value, "glu_gate": glu_gate, "conv_kernel": conv_kernel, "norm_gain": norm_gain, "mix_weight": mix_weight, "residual": residual, "resid_gain": resid_gain, "expert_ids": expert_ids, "route_weight": route_weight, "w_gate": w_gate, "w_up": w_up, "w_down": w_down, "out_gain": out_gain}


EPSILON = 1e-05
LIMIT = 7.0
SLOPE = 1.702

def normalize(values, gain_vector):
    centre = lax.optimization_barrier(jnp.mean(values, axis=-1, keepdims=True))
    spread = lax.optimization_barrier(jnp.mean(jnp.square(values - centre), axis=-1, keepdims=True))
    return (values - centre) * lax.rsqrt(spread + EPSILON) * gain_vector

def slot_layout(route_ids, experts, capacity):
    row_count, top_count = route_ids.shape
    flat_ids = route_ids.reshape(row_count * top_count).astype(jnp.int32)
    onehot = (flat_ids[:, None] == jnp.arange(experts, dtype=jnp.int32)[None, :]).astype(jnp.int32)
    before = jnp.cumsum(onehot, axis=0) - onehot
    slot_rank = lax.optimization_barrier(jnp.sum(before * onehot, axis=1)).astype(jnp.int32)
    position = (flat_ids * capacity + slot_rank).astype(jnp.int32)
    owners = (jnp.arange(row_count * top_count, dtype=jnp.int32) // top_count).astype(jnp.int32)
    slot_table = jnp.full((experts * capacity,), row_count, jnp.int32).at[position].set(owners)
    return (slot_table, position.reshape(row_count, top_count))

def run_expert(operands):
    tokens, gate_matrix, up_matrix, down_matrix = operands
    tokens_wide = tokens.astype(jnp.float32)
    gate_pre = jnp.dot(tokens_wide, gate_matrix.astype(jnp.float32), preferred_element_type=jnp.float32)
    up_pre = jnp.dot(tokens_wide, up_matrix.astype(jnp.float32), preferred_element_type=jnp.float32)
    gated = jnp.minimum(gate_pre, LIMIT)
    upper = jnp.clip(up_pre, -LIMIT, LIMIT)
    activity = ((upper + 1.0) * gated * jax.nn.sigmoid(SLOPE * gated)).astype(jnp.bfloat16)
    quarter = FFE // N_TP
    pieces = activity.reshape(-1, N_TP, quarter).astype(jnp.float32)
    downs = down_matrix.reshape(N_TP, quarter, D).astype(jnp.float32)
    partials = jnp.einsum('rqf,qfd->qrd', pieces, downs).astype(jnp.bfloat16)
    partials = lax.optimization_barrier(partials)
    return lax.optimization_barrier(jnp.sum(partials.astype(jnp.float32), axis=0)).astype(jnp.bfloat16)

def reference(glu_value, glu_gate, conv_kernel, norm_gain, mix_weight, residual, resid_gain, expert_ids, route_weight, w_gate, w_up, w_down, out_gain):
    gated_in = (glu_value.astype(jnp.float32) * jax.nn.sigmoid(glu_gate.astype(jnp.float32))).astype(jnp.bfloat16)
    extended = jnp.pad(gated_in.astype(jnp.float32), ((KERNEL - 1, 0), (0, 0)))
    convolved = jnp.zeros((TOKENS, DC), jnp.float32)
    for offset in range(KERNEL):
        convolved = convolved + conv_kernel[offset] * extended[offset:offset + TOKENS]
    centre = lax.optimization_barrier(jnp.mean(convolved, axis=1, keepdims=True))
    spread = lax.optimization_barrier(jnp.mean(jnp.square(convolved), axis=1, keepdims=True)) - centre * centre
    normed = (convolved - centre) * lax.rsqrt(spread + EPSILON) * norm_gain
    mix_in = jax.nn.silu(normed).astype(jnp.bfloat16)
    mixed_rows = jnp.dot(mix_in, mix_weight, preferred_element_type=jnp.float32)
    hidden = normalize(residual.astype(jnp.float32) + mixed_rows, resid_gain).astype(jnp.bfloat16)
    block_count = N_SP * N_TP
    block_ids = expert_ids.reshape(block_count, BLOCK, TOPK)
    tables, positions = jax.vmap(partial(slot_layout, experts=EXPERTS, capacity=CAP))(block_ids)
    hidden_blocks = hidden.reshape(block_count, BLOCK, D)
    padded = jnp.concatenate([hidden_blocks, jnp.zeros((block_count, 1, D), jnp.bfloat16)], axis=1)
    slot_rows = jax.vmap(partial(jnp.take, axis=0))(padded, tables)
    expert_major = slot_rows.reshape(block_count, EXPERTS, CAP, D).transpose(1, 0, 2, 3)
    expert_major = expert_major.reshape(EXPERTS, block_count * CAP, D)
    outputs = lax.map(run_expert, (expert_major, w_gate, w_up, w_down))
    block_major = outputs.reshape(EXPERTS, block_count, CAP, D).transpose(1, 0, 2, 3)
    block_major = block_major.reshape(block_count, EXPERTS * CAP, D)
    picked = jax.vmap(partial(jnp.take, axis=0))(block_major, positions.reshape(block_count, BLOCK * TOPK))
    picked = picked.reshape(TOKENS, TOPK, D)
    routed_sum = jnp.einsum('tk,tkd->td', route_weight.astype(jnp.float32), picked.astype(jnp.float32))
    return normalize(hidden.astype(jnp.float32) + routed_sum, out_gain).astype(jnp.bfloat16)
```

```python
import jax
import jax.numpy as jnp
from jax import lax
from jax.sharding import PartitionSpec as P

DC = 2048


EPSILON = 1e-05
LIMIT = 7.0
SLOPE = 1.702


def shifted(block, axis, distance):
    devices = range(lax.axis_size(axis))
    route = [(i - distance, i) for i in devices if i - distance in devices]
    return lax.ppermute(block, axis, route)


def copy_for_each(array, axis):
    count = lax.axis_size(axis)
    return lax.all_to_all(
        jnp.broadcast_to(array[None], (count, *array.shape)), axis, 0, 0, tiled=True
    )


def of_everyone(array, axis):
    return copy_for_each(array, axis).sum(axis=0)


def together(arrays, axis):
    ends = [0]
    for a in arrays:
        ends.append(ends[-1] + a.size)
    running = of_everyone(jnp.concatenate([a.ravel() for a in arrays]), axis)
    return tuple((running[b:e].reshape(a.shape) for a, b, e in zip(arrays, ends, ends[1:])))


def cut_along(array, dim, count):
    before, after = (array.shape[:dim], array.shape[dim + 1 :])
    return jnp.moveaxis(array.reshape(*before, count, -1, *after), dim, 0)


def sum_at_owner(array, axis, dim):
    tiles = cut_along(array, dim, lax.axis_size(axis))
    arrived = lax.all_to_all(tiles, axis, split_axis=0, concat_axis=0, tiled=True)
    return arrived.astype(jnp.float32).sum(axis=0)


def in_order(tiles, dim):
    dims = list(tiles.shape[1:])
    dims[dim] *= tiles.shape[0]
    return jnp.moveaxis(tiles, 0, dim).reshape(dims)


def work_in_pieces(array, axis, dim, apply, out_dim):
    size, extent = (lax.axis_size(axis), array.shape[dim])
    count = 2 if extent % 2 == 0 else 1
    done, length = ([], extent // count)
    for k in range(count):
        section = lax.slice_in_dim(array, k * length, (k + 1) * length, axis=dim)
        starts = jnp.arange(size) * extent + k * length
        done.append(jax.vmap(apply)(lax.all_gather(section, axis), starts))
    return in_order(jnp.concatenate(done, axis=out_dim + 1), out_dim)


def normalize(values, gain_vector):
    centre = jnp.mean(values, axis=-1, keepdims=True)
    spread = jnp.mean(jnp.square(values - centre), axis=-1, keepdims=True)
    return (values - centre) * lax.rsqrt(spread + EPSILON) * gain_vector


def swap_route(nearby):
    count, size = (lax.axis_size("sp"), lax.axis_size("tp"))
    route = []
    for s in range(count):
        for t in range(size):
            partner = t ^ 1 if (s % 2 == 0) == nearby else size - 1 - t
            route.append((s * size + t, s * size + partner))
    return route


def weight_route():
    return swap_route(True)


def cross_route():
    return swap_route(False)


def slot_layout(route_ids, experts, capacity):
    row_count, top_count = route_ids.shape
    flat_ids = route_ids.reshape(row_count * top_count)
    onehot = (flat_ids[:, None] == jnp.arange(experts, dtype=jnp.int32)[None, :]).astype(jnp.int32)
    before = jnp.cumsum(onehot, axis=0) - onehot
    slot_rank = jnp.sum(before * onehot, axis=1)
    position = flat_ids * capacity + slot_rank
    owners = jnp.arange(row_count * top_count, dtype=jnp.int32) // top_count
    slot_table = jnp.full((experts * capacity,), row_count, jnp.int32).at[position].set(owners)
    return (slot_table, position.reshape(row_count, top_count))


def expert_activity(tokens, gate_matrix, up_matrix):
    gate_pre = jnp.dot(tokens, gate_matrix, preferred_element_type=jnp.float32)
    up_pre = jnp.dot(tokens, up_matrix, preferred_element_type=jnp.float32)
    gated = jnp.minimum(gate_pre, LIMIT)
    upper = jnp.clip(up_pre, -LIMIT, LIMIT)
    return ((upper + 1.0) * gated * jax.nn.sigmoid(SLOPE * gated)).astype(jnp.bfloat16)


def shards(
    glu_value,
    glu_gate,
    conv_kernel,
    norm_gain,
    mix_weight,
    residual,
    resid_gain,
    expert_ids,
    route_weight,
    w_gate,
    w_up,
    w_down,
    out_gain,
):
    gated_in = (
        glu_value.astype(jnp.float32) * jax.nn.sigmoid(glu_gate.astype(jnp.float32))
    ).astype(jnp.bfloat16)
    reach_back = conv_kernel.shape[0] - 1
    length = gated_in.shape[0]
    before_rows = shifted(gated_in[length - reach_back :], "sp", 1)
    extended = jnp.concatenate([before_rows, gated_in], axis=0).astype(jnp.float32)
    convolved = jnp.zeros(gated_in.shape, jnp.float32)
    for offset in range(reach_back + 1):
        convolved = convolved + conv_kernel[offset] * extended[offset : offset + length]
    channel_sum, squares = together(
        (jnp.sum(convolved, axis=1), jnp.sum(convolved * convolved, axis=1)), "tp"
    )
    centre = channel_sum / DC
    spread = squares / DC - centre * centre
    normed = (convolved - centre[:, None]) * lax.rsqrt(spread[:, None] + EPSILON) * norm_gain
    mix_in = jax.nn.silu(normed).astype(jnp.bfloat16)
    tp_count = lax.axis_size("tp")
    own_count = length // tp_count
    section = mix_in
    mixed_rows = sum_at_owner(
        jnp.dot(section, mix_weight, preferred_element_type=jnp.float32).astype(jnp.bfloat16),
        "tp",
        0,
    )
    hidden = normalize(residual.astype(jnp.float32) + mixed_rows, resid_gain).astype(jnp.bfloat16)
    experts = lax.axis_size("sp")
    top_count = expert_ids.shape[1]
    capacity = 2 * own_count * top_count // experts
    width = hidden.shape[1]
    gate_local = w_gate[0]
    up_local = w_up[0]
    down_local = w_down[0]

    gate_other, up_other, down_other = (
        lax.ppermute(w, ("sp", "tp"), weight_route()) for w in (gate_local, up_local, down_local)
    )

    def half_experts(rows):
        own = expert_activity(rows, gate_local, up_local)
        other = expert_activity(rows, gate_other, up_other)
        return jnp.dot(own, down_local, preferred_element_type=jnp.float32) + jnp.dot(
            other, down_other, preferred_element_type=jnp.float32
        )

    own_table, positions = slot_layout(expert_ids, experts, capacity)
    padded = jnp.concatenate([hidden, jnp.zeros((1, width), jnp.bfloat16)], axis=0)
    dispatched = padded[own_table].reshape(experts, capacity, width)
    arrived = lax.all_to_all(dispatched, "sp", split_axis=0, concat_axis=0, tiled=True)
    arrived = arrived.reshape(experts * capacity, width)
    crossed = lax.ppermute(arrived, ("sp", "tp"), cross_route())
    sent = half_experts(crossed)
    kept = half_experts(arrived)
    back = lax.ppermute(sent.astype(jnp.bfloat16), ("sp", "tp"), cross_route())
    expert_out = (kept + back.astype(jnp.float32)).astype(jnp.bfloat16)
    expert_out = expert_out.reshape(experts, capacity, width)
    returned_rows = lax.all_to_all(expert_out, "sp", split_axis=0, concat_axis=0, tiled=True)
    picked = returned_rows.reshape(experts * capacity, width)[positions.reshape(-1)]
    picked = picked.reshape(own_count, top_count, width)
    routed_sum = jnp.einsum("tk,tkd->td", route_weight, picked.astype(jnp.float32))
    return normalize(hidden.astype(jnp.float32) + routed_sum, out_gain).astype(jnp.bfloat16)


def solution(mesh):
    in_specs = (
        P("sp", "tp"),
        P("sp", "tp"),
        P(None, "tp"),
        P("tp"),
        P("tp", None),
        P(("sp", "tp"), None),
        P(),
        P(("sp", "tp"), None),
        P(("sp", "tp"), None),
        P("sp", None, "tp"),
        P("sp", None, "tp"),
        P("sp", "tp", None),
        P(),
    )
    out_specs = P(("sp", "tp"), None)
    return jax.shard_map(shards, mesh=mesh, in_specs=in_specs, out_specs=out_specs, check_vma=False)
```

```python
import jax
import jax.numpy as jnp
from jax import lax
from jax.experimental import pallas as pl
from jax.experimental.pallas import tpu as pltpu
from jax.sharding import PartitionSpec as P

DC = 2048


EPSILON = 1e-05
LIMIT = 7.0
SLOPE = 1.702


def shifted(block, axis, distance):
    devices = range(lax.axis_size(axis))
    route = [(i - distance, i) for i in devices if i - distance in devices]
    return lax.ppermute(block, axis, route)


def copy_for_each(array, axis):
    count = lax.axis_size(axis)
    return lax.all_to_all(
        jnp.broadcast_to(array[None], (count, *array.shape)), axis, 0, 0, tiled=True
    )


def of_everyone(array, axis):
    return copy_for_each(array, axis).sum(axis=0)


def together(arrays, axis):
    ends = [0]
    for a in arrays:
        ends.append(ends[-1] + a.size)
    running = of_everyone(jnp.concatenate([a.ravel() for a in arrays]), axis)
    return tuple((running[b:e].reshape(a.shape) for a, b, e in zip(arrays, ends, ends[1:])))


def cut_along(array, dim, count):
    before, after = (array.shape[:dim], array.shape[dim + 1 :])
    return jnp.moveaxis(array.reshape(*before, count, -1, *after), dim, 0)


def sum_at_owner(array, axis, dim):
    tiles = cut_along(array, dim, lax.axis_size(axis))
    arrived = lax.all_to_all(tiles, axis, split_axis=0, concat_axis=0, tiled=True)
    return arrived.astype(jnp.float32).sum(axis=0)


def in_order(tiles, dim):
    dims = list(tiles.shape[1:])
    dims[dim] *= tiles.shape[0]
    return jnp.moveaxis(tiles, 0, dim).reshape(dims)


def normalize(values, gain_vector):
    centre = jnp.mean(values, axis=-1, keepdims=True)
    spread = jnp.mean(jnp.square(values - centre), axis=-1, keepdims=True)
    return (values - centre) * lax.rsqrt(spread + EPSILON) * gain_vector


Z, Y, CORES = 8, 4, 2
PLANE = Y * CORES
GROUPS = 4
PEERS = 2 * PLANE
SELF = 3 * PEERS + PLANE
CAP = 8
TILE = 256
MESH = pl.DeviceIdType.MESH


def position():
    sp, tp = lax.axis_index("sp"), lax.axis_index("tp")
    z, y, core = sp // PLANE, (sp // CORES) % Y, sp % CORES
    near, far = tp + 1 - 2 * (tp % 2), 3 - tp
    weight_partner = near * (1 - core) + far * core
    row_partner = near * core + far * (1 - core)
    return sp, tp, z, y, core, weight_partner, row_partner


def step_along_z(group, half):
    return (group + 1) if half == 0 else (7 - group) * (1 - (group + 1) // 4)


def peer_at(z, y, core, dz, r, sign):
    return ((z + sign * dz + Z) % Z) * PLANE + ((y + sign * (r // 2) + Y) % Y) * CORES + (core + r % 2) % CORES


def wait_for(ref, sem):
    pltpu.make_async_copy(ref, ref, sem).wait()


def routed_kernel(
    slots, w_gate, w_up, w_down, ret,
    gate_v, up_v, down_v, recv, xrecv, rows_v, act_v, kept, xsend, xret, fin,
    d_send, d_recv, x_send, x_recv, b_send, b_recv, r_send, r_recv, w_send, w_recv, l_sem,
):
    sp, tp, z, y, core, weight_partner, row_partner = position()
    barrier = pltpu.get_barrier_semaphore()

    def greet(i, _):
        other = lax.rem(sp + i, Z * PLANE)
        pl.semaphore_signal(barrier, inc=1, device_id=(other, tp), device_id_type=MESH)
        return 0

    lax.fori_loop(1, Z * PLANE, greet, 0)
    for partner in (weight_partner, row_partner):
        pl.semaphore_signal(barrier, inc=1, device_id=(sp, partner), device_id_type=MESH)
    width = w_down.shape[2]
    half_units = w_down.shape[1]
    loads = [
        pltpu.make_async_copy(w_gate.at[0], gate_v.at[0], l_sem.at[0]),
        pltpu.make_async_copy(w_up.at[0], up_v.at[0], l_sem.at[1]),
        pltpu.make_async_copy(w_down.at[0], down_v.at[0:half_units], l_sem.at[2]),
    ]
    for load in loads:
        load.start()
    pltpu.make_async_copy(slots.at[sp], recv.at[SELF], d_recv.at[SELF]).start()
    pl.semaphore_wait(barrier, Z * PLANE + 1)

    def swap(i, src, dst):
        return pltpu.make_async_remote_copy(
            src_ref=src, dst_ref=dst, send_sem=w_send.at[i], recv_sem=w_recv.at[i],
            device_id=(sp, weight_partner), device_id_type=MESH,
        )

    swaps = [
        swap(0, w_gate.at[0], gate_v.at[1]),
        swap(1, w_up.at[0], up_v.at[1]),
        swap(2, w_down.at[0], down_v.at[half_units : 2 * half_units]),
    ]
    for group in range(GROUPS):
        for half in range(2):
            dz = step_along_z(group, half)
            base = group * PEERS + half * PLANE

            def send(r, _, dz=dz, base=base):
                other = peer_at(z, y, core, dz, r, 1)
                pltpu.make_async_remote_copy(
                    src_ref=slots.at[other], dst_ref=recv.at[base + r],
                    send_sem=d_send.at[base + r], recv_sem=d_recv.at[base + r],
                    device_id=(other, tp), device_id_type=MESH,
                ).start()
                return 0

            lax.fori_loop(1 if base == SELF else 0, PLANE, send, 0)
    for s in swaps:
        s.start()

    def cross(c, src, dst, send_sem, recv_sem):
        return pltpu.make_async_remote_copy(
            src_ref=src.at[pl.ds(c * PEERS, PEERS)], dst_ref=dst.at[pl.ds(c * PEERS, PEERS)],
            send_sem=send_sem.at[c], recv_sem=recv_sem.at[c],
            device_id=(sp, row_partner), device_id_type=MESH,
        )

    count = PEERS * CAP

    def stage(step, _):
        @pl.when(step < GROUPS)
        def arrive():
            def one(r, _):
                wait_for(recv.at[step * PEERS + r], d_recv.at[step * PEERS + r])
                return 0

            lax.fori_loop(0, PEERS, one, 0)
            cross(step, recv, xrecv, x_send, x_recv).start()

        @pl.when(step == 1)
        def weights():
            for load in loads:
                load.wait()
            for s in swaps:
                s.wait()

        @pl.when((step >= 1) & (step <= GROUPS))
        def compute():
            c = step - 1
            cross(c, recv, xrecv, x_send, x_recv).wait_recv()
            at = pl.ds(c * PEERS, PEERS)
            rows_v[0:count] = recv[at].astype(jnp.float32).reshape(count, width).astype(jnp.bfloat16)
            rows_v[count : 2 * count] = xrecv[at].astype(jnp.float32).reshape(count, width).astype(jnp.bfloat16)

            def activate(j, _):
                half, col = j // 2, pl.multiple_of((j % 2) * TILE, TILE)
                g = jnp.dot(rows_v[...], gate_v[half, :, pl.ds(col, TILE)], preferred_element_type=jnp.float32)
                u = jnp.dot(rows_v[...], up_v[half, :, pl.ds(col, TILE)], preferred_element_type=jnp.float32)
                g = jnp.minimum(g, LIMIT)
                u = jnp.clip(u, -LIMIT, LIMIT)
                act = (u + 1.0) * g * jax.nn.sigmoid(SLOPE * g)
                act_v[:, pl.ds(pl.multiple_of(j * TILE, TILE), TILE)] = act.astype(jnp.bfloat16)
                return 0

            lax.fori_loop(0, 2 * half_units // TILE, activate, 0)

            def project(n, _):
                cols = pl.ds(pl.multiple_of(n * TILE, TILE), TILE)
                out = jnp.dot(act_v[...], down_v[:, cols], preferred_element_type=jnp.float32)
                kept[c % 2, :, cols] = out[0:count]
                xsend[at, :, cols] = out[count : 2 * count].reshape(PEERS, CAP, TILE).astype(jnp.bfloat16)
                return 0

            lax.fori_loop(0, width // TILE, project, 0)
            cross(c, xsend, xret, b_send, b_recv).start()

        @pl.when(step >= 2)
        def give_back():
            c = step - 2
            cross(c, xsend, xret, b_send, b_recv).wait_recv()
            at = pl.ds(c * PEERS, PEERS)
            total = kept[c % 2].reshape(PEERS, CAP, width) + xret[at].astype(jnp.float32)
            fin[at] = total.astype(jnp.bfloat16)
            for half in range(2):
                dz = step_along_z(c, half)

                def send(r, _, dz=dz, half=half):
                    k = c * PEERS + half * PLANE + r
                    other = peer_at(z, y, core, dz, r, -1)

                    @pl.when(k != SELF)
                    def away():
                        pltpu.make_async_remote_copy(
                            src_ref=fin.at[k], dst_ref=ret.at[sp],
                            send_sem=r_send.at[k], recv_sem=r_recv.at[k],
                            device_id=(other, tp), device_id_type=MESH,
                        ).start()

                    @pl.when(k == SELF)
                    def here():
                        pltpu.make_async_copy(fin.at[k], ret.at[sp], r_recv.at[k]).start()

                    return 0

                lax.fori_loop(0, PLANE, send, 0)

        return 0

    lax.fori_loop(0, GROUPS + 2, stage, 0)

    def finish(k, _):
        wait_for(ret.at[k], r_recv.at[k])

        @pl.when(k != SELF)
        def away():
            wait_for(recv.at[k], d_send.at[k])
            wait_for(fin.at[k], r_send.at[k])

        return 0

    lax.fori_loop(0, Z * PLANE, finish, 0)
    for c in range(GROUPS):
        cross(c, recv, xrecv, x_send, x_recv).wait_send()
        cross(c, xsend, xret, b_send, b_recv).wait_send()


def routed(slots, w_gate, w_up, w_down):
    experts, cap, width = slots.shape
    units = w_down.shape[1]
    count = PEERS * CAP
    dma = pltpu.SemaphoreType.DMA
    vmem, hbm = pl.BlockSpec(memory_space=pltpu.VMEM), pl.BlockSpec(memory_space=pl.ANY)
    moved = pltpu.VMEM(slots.shape, jnp.bfloat16)
    return pl.pallas_call(
        routed_kernel,
        out_shape=jax.ShapeDtypeStruct(slots.shape, jnp.bfloat16),
        in_specs=[vmem, hbm, hbm, hbm],
        out_specs=vmem,
        scratch_shapes=[
            pltpu.VMEM((2, width, units), jnp.bfloat16),
            pltpu.VMEM((2, width, units), jnp.bfloat16),
            pltpu.VMEM((2 * units, width), jnp.bfloat16),
            moved,
            moved,
            pltpu.VMEM((2 * count, width), jnp.bfloat16),
            pltpu.VMEM((2 * count, 2 * units), jnp.bfloat16),
            pltpu.VMEM((2, count, width), jnp.float32),
            moved,
            moved,
            moved,
            dma((experts,)), dma((experts,)),
            dma((GROUPS,)), dma((GROUPS,)),
            dma((GROUPS,)), dma((GROUPS,)),
            dma((experts,)), dma((experts,)),
            dma((3,)), dma((3,)), dma((3,)),
        ],
        compiler_params=pltpu.CompilerParams(
            collective_id=0, has_side_effects=True, vmem_limit_bytes=56 * 2**20
        ),
        name="routed",
    )(slots, w_gate, w_up, w_down)


def slot_positions(route_ids, capacity):
    flat = route_ids.reshape(-1)
    order = jnp.arange(flat.shape[0], dtype=jnp.int32)
    earlier = (flat[:, None] == flat[None, :]) & (order[None, :] < order[:, None])
    rank = jnp.sum(earlier.astype(jnp.int32), axis=1)
    return (flat * capacity + rank).reshape(route_ids.shape)


def shards(
    glu_value,
    glu_gate,
    conv_kernel,
    norm_gain,
    mix_weight,
    residual,
    resid_gain,
    expert_ids,
    route_weight,
    w_gate,
    w_up,
    w_down,
    out_gain,
):
    gated_in = (
        glu_value.astype(jnp.float32) * jax.nn.sigmoid(glu_gate.astype(jnp.float32))
    ).astype(jnp.bfloat16)
    reach_back = conv_kernel.shape[0] - 1
    length = gated_in.shape[0]
    before_rows = shifted(gated_in[length - reach_back :], "sp", 1)
    extended = jnp.concatenate([before_rows, gated_in], axis=0).astype(jnp.float32)
    convolved = jnp.zeros(gated_in.shape, jnp.float32)
    for offset in range(reach_back + 1):
        convolved = convolved + conv_kernel[offset] * extended[offset : offset + length]
    channel_sum, squares = together(
        (jnp.sum(convolved, axis=1), jnp.sum(convolved * convolved, axis=1)), "tp"
    )
    centre = channel_sum / DC
    spread = squares / DC - centre * centre
    normed = (convolved - centre[:, None]) * lax.rsqrt(spread[:, None] + EPSILON) * norm_gain
    mix_in = jax.nn.silu(normed).astype(jnp.bfloat16)
    tp_count = lax.axis_size("tp")
    own_count = length // tp_count
    section = mix_in
    mixed_rows = sum_at_owner(
        jnp.dot(section, mix_weight, preferred_element_type=jnp.float32).astype(jnp.bfloat16),
        "tp",
        0,
    )
    hidden = normalize(residual.astype(jnp.float32) + mixed_rows, resid_gain).astype(jnp.bfloat16)
    experts = lax.axis_size("sp")
    width = hidden.shape[1]
    positions = slot_positions(expert_ids, CAP)
    places = jnp.arange(experts * CAP, dtype=jnp.int32)
    named = positions[:, :, None] == places
    held = jnp.any(named, axis=1).astype(jnp.bfloat16)
    slots = lax.dot_general(held, hidden, (((0,), (0,)), ((), ())), preferred_element_type=jnp.float32)
    slots = slots.astype(jnp.bfloat16).reshape(experts, CAP, width)
    returned = routed(slots, w_gate, w_up, w_down).reshape(experts * CAP, width)
    share = jnp.sum(jnp.where(named, route_weight[:, :, None], 0.0), axis=1)
    share_high = share.astype(jnp.bfloat16)
    share_low = (share - share_high.astype(jnp.float32)).astype(jnp.bfloat16)
    routed_sum = jnp.dot(share_high, returned, preferred_element_type=jnp.float32) + jnp.dot(
        share_low, returned, preferred_element_type=jnp.float32
    )
    return normalize(hidden.astype(jnp.float32) + routed_sum, out_gain).astype(jnp.bfloat16)


def solution(mesh):
    in_specs = (
        P("sp", "tp"),
        P("sp", "tp"),
        P(None, "tp"),
        P("tp"),
        P("tp", None),
        P(("sp", "tp"), None),
        P(),
        P(("sp", "tp"), None),
        P(("sp", "tp"), None),
        P("sp", None, "tp"),
        P("sp", None, "tp"),
        P("sp", "tp", None),
        P(),
    )
    out_specs = P(("sp", "tp"), None)
    return jax.shard_map(shards, mesh=mesh, in_specs=in_specs, out_specs=out_specs, check_vma=False)
```

```python
import jax
import jax.numpy as jnp
from jax import lax
from jax.experimental import pallas as pl
from jax.experimental.pallas import tpu as pltpu
from jax.sharding import PartitionSpec as P

DC = 2048
EPSILON = 1e-05
LIMIT = 7.0
SLOPE = 1.702
Z, Y, CORES, N_TP = 8, 4, 2, 4
PLANE = Y * CORES
N_SP = Z * PLANE
GROUPS = 4
PEERS = 2 * PLANE
SELF_GROUP = 3
SELF = SELF_GROUP * PEERS + PLANE
CAP = 8
TILE = 256
LANES = 128
TAPS = 31
HALO = 32
ROWS = 512
BLOCK = 128
STRIPE = 64
MESH = pl.DeviceIdType.MESH
F32, BF16 = jnp.float32, jnp.bfloat16


def normalize(values, gain_vector):
    centre = jnp.mean(values, axis=-1, keepdims=True)
    spread = jnp.mean(jnp.square(values - centre), axis=-1, keepdims=True)
    return (values - centre) * lax.rsqrt(spread + EPSILON) * gain_vector


def position():
    sp, tp = lax.axis_index("sp"), lax.axis_index("tp")
    z, y, core = sp // PLANE, (sp // CORES) % Y, sp % CORES
    near, far = tp + 1 - 2 * (tp % 2), 3 - tp
    weight_partner = near * (1 - core) + far * core
    row_partner = near * core + far * (1 - core)
    return sp, tp, z, y, core, weight_partner, row_partner


def step_along_z(group, half):
    return (group + 1) if half == 0 else (7 - group) * (1 - (group + 1) // 4)


def peer_at(z, y, core, dz, r, sign):
    return ((z + sign * dz + Z) % Z) * PLANE + ((y + sign * (r // 2) + Y) % Y) * CORES + (core + r % 2) % CORES


def wait_for(ref, sem):
    pltpu.make_async_copy(ref, ref, sem).wait()


def layer_kernel(
    value, gate, taps, norm_gain, residual, resid_gain, out_gain, ids, weights,
    mix_weight, w_gate, w_up, w_down,
    out,
    ext, halo_send, halo_recv, conv_v, stat_cols, stat_rows, stats_send, stats_recv, mix_in, mix_v,
    a_send_v, a_recv_v, b_send_v, b_recv_v, acc, hidden, held, share, slots, ret,
    gate_v, up_v, down_v, recv, xrecv, rows_v, act_v, kept, xsend, xret, fin,
    d_send, d_recv, x_send, x_recv, b_send, b_recv, r_send, r_recv, w_send, w_recv, l_sem,
    h_sem, s_send, s_recv, ra_send, ra_recv, rb_send, rb_recv,
):
    sp, tp, z, y, core, weight_partner, row_partner = position()
    barrier = pltpu.get_barrier_semaphore()

    def greet(i, _):
        other = lax.rem(sp + i, N_SP)
        pl.semaphore_signal(barrier, inc=1, device_id=(other, tp), device_id_type=MESH)
        return 0

    lax.fori_loop(1, N_SP, greet, 0)
    for i in range(1, N_TP):
        pl.semaphore_signal(barrier, inc=1, device_id=(sp, (tp + i) % N_TP), device_id_type=MESH)
    width = w_down.shape[2]
    half_units = w_down.shape[1]
    channels = value.shape[1]
    loads = [
        pltpu.make_async_copy(mix_weight, mix_v, l_sem.at[3]),
        pltpu.make_async_copy(w_gate.at[0], gate_v.at[0], l_sem.at[0]),
        pltpu.make_async_copy(w_up.at[0], up_v.at[0], l_sem.at[1]),
        pltpu.make_async_copy(w_down.at[0], down_v.at[0:half_units], l_sem.at[2]),
    ]
    for load in loads:
        load.start()

    lane_groups = channels // LANES

    def gated(rows, cols):
        product = value[rows, cols].astype(F32) * jax.nn.sigmoid(gate[rows, cols].astype(F32))
        return product.astype(BF16)

    for g in range(lane_groups):
        halo_send[g] = gated(pl.ds(ROWS - HALO, HALO), pl.ds(g * LANES, LANES))

    def gate_rows(i, _):
        for g in range(lane_groups):
            at = pl.ds(pl.multiple_of(i * STRIPE, STRIPE), STRIPE)
            to = pl.ds(pl.multiple_of(i * STRIPE + HALO, HALO), STRIPE)
            ext[g, to] = gated(at, pl.ds(g * LANES, LANES)).astype(F32)
        return 0

    lax.fori_loop(0, ROWS // STRIPE, gate_rows, 0)
    pl.semaphore_wait(barrier, N_SP - 1 + N_TP - 1)
    halo_copy = pltpu.make_async_remote_copy(
        src_ref=halo_send, dst_ref=halo_recv, send_sem=h_sem.at[0], recv_sem=h_sem.at[1],
        device_id=(lax.rem(sp + 1, N_SP), tp), device_id_type=MESH,
    )
    halo_copy.start()

    def swap(i, src, dst):
        return pltpu.make_async_remote_copy(
            src_ref=src, dst_ref=dst, send_sem=w_send.at[i], recv_sem=w_recv.at[i],
            device_id=(sp, weight_partner), device_id_type=MESH,
        )

    def rows_of(ref, first, last):
        return ref.at[pl.ds(first, last - first)]

    cuts = (0, 512, 1024, 2048)
    swaps = [
        swap(i, w_gate.at[0, pl.ds(f, l - f)], gate_v.at[1, pl.ds(f, l - f)])
        for i, (f, l) in enumerate(zip(cuts, cuts[1:]))
    ] + [
        swap(3, w_up.at[0], up_v.at[1]),
        swap(4, w_down.at[0], down_v.at[half_units : 2 * half_units]),
    ]
    swaps[0].start()

    lane = lax.broadcasted_iota(jnp.int32, (STRIPE, LANES), 1)

    def convolve(i):
        first = pl.multiple_of(i * STRIPE, STRIPE)
        total, square = jnp.zeros((STRIPE, LANES), F32), jnp.zeros((STRIPE, LANES), F32)
        for g in range(lane_groups):
            sums = jnp.zeros((STRIPE, LANES), F32)
            for k in range(TAPS):
                tap = taps[k : k + 1, g * LANES : (g + 1) * LANES]
                sums = sums + tap * ext[g, pl.ds(first + (HALO - TAPS + 1 + k), STRIPE)]
            conv_v[g, pl.ds(first, STRIPE)] = sums
            total, square = total + sums, square + sums * sums
        total = jnp.sum(total, axis=1, keepdims=True)
        square = jnp.sum(square, axis=1, keepdims=True)
        stat_cols[pl.ds(first, STRIPE)] = jnp.where(lane == 0, total, jnp.where(lane == 1, square, 0.0))

    def convolve_step(i, _):
        convolve(i)
        return 0

    lax.fori_loop(1, ROWS // STRIPE, convolve_step, 0)
    halo_copy.wait_recv()
    for g in range(lane_groups):
        ext[g, 0:HALO] = jnp.where(sp > 0, halo_recv[g].astype(F32), 0.0)
    convolve(0)
    for i in range(ROWS // LANES):
        at = slice(i * LANES, (i + 1) * LANES)
        stats_send[:, at] = jnp.transpose(stat_cols[at, :])[0:8]
    stat_copies = [
        pltpu.make_async_remote_copy(
            src_ref=stats_send, dst_ref=stats_recv.at[j - 1], send_sem=s_send.at[j - 1], recv_sem=s_recv.at[j - 1],
            device_id=(sp, (tp + j) % N_TP), device_id_type=MESH,
        )
        for j in (2, 1, 3)
    ]
    for c in stat_copies:
        c.start()
    swaps[1].start()

    experts = N_SP
    spot = lax.broadcasted_iota(jnp.int32, (experts, BLOCK), 0)
    one = [(spot == ids[j : j + 1, :]).astype(BF16) for j in range(2)]
    before = lax.broadcasted_iota(jnp.int32, (BLOCK, BLOCK), 0) < lax.broadcasted_iota(jnp.int32, (BLOCK, BLOCK), 1)
    earlier = jnp.dot(one[0] + one[1], before.astype(BF16), preferred_element_type=F32)
    owner = lax.broadcasted_iota(jnp.int32, (experts * CAP, experts), 0) // CAP
    spread_out = (owner == lax.broadcasted_iota(jnp.int32, (experts * CAP, experts), 1)).astype(BF16)
    rank = jnp.dot(spread_out, earlier.astype(BF16), preferred_element_type=F32)
    in_rank = rank == (lax.broadcasted_iota(jnp.int32, (experts * CAP, BLOCK), 0) % CAP).astype(F32)
    hits = [
        jnp.where(in_rank, jnp.dot(spread_out, o, preferred_element_type=F32), 0.0) for o in one
    ]
    held[...] = (hits[0] + hits[1]).astype(BF16)
    shares = hits[0] * weights[0:1, :] + hits[1] * weights[1:2, :]
    for i in range(experts * CAP // LANES):
        at = slice(i * LANES, (i + 1) * LANES)
        part = jnp.transpose(shares[at, :])
        high = part.astype(BF16)
        share[0:BLOCK, at] = high
        share[BLOCK : 2 * BLOCK, at] = (part - high.astype(F32)).astype(BF16)
    stat_rows[...] = jnp.zeros_like(stat_rows)

    for c in stat_copies:
        c.wait_recv()
    sums = stats_send[...] + stats_recv[0] + stats_recv[1] + stats_recv[2]
    centre = sums[0:1] / DC
    scale = lax.rsqrt(sums[1:2] / DC - centre * centre + EPSILON)
    stat_rows[0:1] = centre
    stat_rows[1:2] = scale

    loads[0].wait()

    def mix_rows(b):
        at = pl.ds(pl.multiple_of(b * BLOCK, BLOCK), BLOCK)
        columns = jnp.transpose(stat_rows[:, at])
        for g in range(lane_groups):
            lanes = slice(g * LANES, (g + 1) * LANES)
            v = (conv_v[g, at] - columns[:, 0:1]) * columns[:, 1:2] * norm_gain[:, lanes]
            mix_in[at, lanes] = (v / (1.0 + jnp.exp(-v))).astype(BF16)

    half_width = width // 2

    def project_rows(b, half, into):
        at = pl.ds(pl.multiple_of(b * BLOCK, BLOCK), BLOCK)

        def one_tile(n, _):
            col = pl.multiple_of(n * TILE, TILE)
            cols = pl.ds(pl.multiple_of(half * half_width + n * TILE, TILE), TILE)
            into(pl.ds(col, TILE), jnp.dot(mix_in[at, :], mix_v[:, cols], preferred_element_type=F32))
            return 0

        lax.fori_loop(0, half_width // TILE, one_tile, 0)

    def to_neighbour(src, dst, send_sem, recv_sem, side):
        return pltpu.make_async_remote_copy(
            src_ref=src, dst_ref=dst, send_sem=send_sem, recv_sem=recv_sem,
            device_id=(sp, (tp + (1 if side == 0 else N_TP - 1)) % N_TP), device_id_type=MESH,
        )

    far_copies = [
        to_neighbour(a_send_v.at[i], a_recv_v.at[i], ra_send.at[i], ra_recv.at[i], i) for i in range(2)
    ]
    near_copies = [
        [
            to_neighbour(
                b_send_v.at[i, h], b_recv_v.at[i, h], rb_send.at[2 * i + h], rb_recv.at[2 * i + h], i
            )
            for h in range(2)
        ]
        for i in range(2)
    ]
    far = (tp + 2) % N_TP
    sides = [(tp + 1) % N_TP, (tp + N_TP - 1) % N_TP]
    mix_rows(far)
    for i in range(2):

        def keep(cols, product, i=i):
            a_send_v[i, :, cols] = product.astype(BF16)

        project_rows(far, i, keep)
        far_copies[i].start()
    for i in range(2):
        mix_rows(sides[i])

        def keep(cols, product, i=i):
            b_send_v[i, 1 - i, :, cols] = product.astype(BF16)

        project_rows(sides[i], 1 - i, keep)
        near_copies[i][1 - i].start()
    for i in range(2):
        far_copies[i].wait_recv()

        def keep(cols, product, i=i):
            b_send_v[i, i, :, cols] = (product + a_recv_v[i, :, cols].astype(F32)).astype(BF16)

        project_rows(sides[i], i, keep)
        near_copies[i][i].start()
    for s in swaps[2:]:
        s.start()
    mix_rows(tp)
    for h in range(2):

        def keep(cols, product, h=h):
            acc[h, :, cols] = product

        project_rows(tp, h, keep)
    for i in range(2):
        near_copies[i][1 - i].wait_recv()
    for i in range(2):
        near_copies[i][i].wait_recv()

    strip = 16

    def norm_rows(i, _):
        at = pl.ds(pl.multiple_of(i * strip, strip), strip)
        halves = [
            acc[h, at] + b_recv_v[0, h, at].astype(F32) + b_recv_v[1, h, at].astype(F32) for h in range(2)
        ]
        total = jnp.concatenate(halves, axis=1) + residual[at].astype(F32)
        hidden[at] = normalize(total, resid_gain[...]).astype(BF16)
        return 0

    lax.fori_loop(0, BLOCK // strip, norm_rows, 0)

    def fill_slots(n, _):
        cols = pl.ds(pl.multiple_of(n * TILE, TILE), TILE)
        picked = jnp.dot(held[...], hidden[:, cols], preferred_element_type=F32)
        slots[:, :, cols] = picked.reshape(experts, CAP, TILE).astype(BF16)
        return 0

    lax.fori_loop(0, width // TILE, fill_slots, 0)

    pltpu.make_async_copy(slots.at[sp], recv.at[SELF], d_recv.at[SELF]).start()
    for group in range(GROUPS):
        for half in range(2):
            dz = step_along_z(group, half)
            base = group * PEERS + half * PLANE

            def send(r, _, dz=dz, base=base):
                other = peer_at(z, y, core, dz, r, 1)
                pltpu.make_async_remote_copy(
                    src_ref=slots.at[other], dst_ref=recv.at[base + r],
                    send_sem=d_send.at[base + r], recv_sem=d_recv.at[base + r],
                    device_id=(other, tp), device_id_type=MESH,
                ).start()
                return 0

            lax.fori_loop(1 if base == SELF else 0, PLANE, send, 0)
    def cross(c, src, dst, send_sem, recv_sem):
        return pltpu.make_async_remote_copy(
            src_ref=src.at[pl.ds(c * PEERS, PEERS)], dst_ref=dst.at[pl.ds(c * PEERS, PEERS)],
            send_sem=send_sem.at[c], recv_sem=recv_sem.at[c],
            device_id=(sp, row_partner), device_id_type=MESH,
        )

    count = PEERS * CAP

    def stage(step, _):
        @pl.when(step < GROUPS)
        def arrive():
            def one(r, _):
                wait_for(recv.at[step * PEERS + r], d_recv.at[step * PEERS + r])
                return 0

            lax.fori_loop(0, PEERS, one, 0)
            cross(step, recv, xrecv, x_send, x_recv).start()

        @pl.when(step == 0)
        def gate_weights():
            for load in loads[1:]:
                load.wait()
            for s in swaps[:-1]:
                s.wait_recv()

        @pl.when((step >= 1) & (step <= GROUPS))
        def compute():
            c = step - 1
            cross(c, recv, xrecv, x_send, x_recv).wait_recv()
            at = pl.ds(c * PEERS, PEERS)
            rows_v[0:count] = recv[at].astype(jnp.float32).reshape(count, width).astype(jnp.bfloat16)
            rows_v[count : 2 * count] = xrecv[at].astype(jnp.float32).reshape(count, width).astype(jnp.bfloat16)

            def activate(j, _):
                half, col = j // 2, pl.multiple_of((j % 2) * TILE, TILE)
                g = jnp.dot(rows_v[...], gate_v[half, :, pl.ds(col, TILE)], preferred_element_type=jnp.float32)
                u = jnp.dot(rows_v[...], up_v[half, :, pl.ds(col, TILE)], preferred_element_type=jnp.float32)
                g = jnp.minimum(g, LIMIT)
                u = jnp.clip(u, -LIMIT, LIMIT)
                act = (u + 1.0) * g * jax.nn.sigmoid(SLOPE * g)
                act_v[:, pl.ds(pl.multiple_of(j * TILE, TILE), TILE)] = act.astype(jnp.bfloat16)
                return 0

            lax.fori_loop(0, 2 * half_units // TILE, activate, 0)

            @pl.when(step == 1)
            def down_weights():
                swaps[-1].wait_recv()


            def project(n, _):
                cols = pl.ds(pl.multiple_of(n * TILE, TILE), TILE)
                out = jnp.dot(act_v[...], down_v[:, cols], preferred_element_type=jnp.float32)
                kept[c % 2, :, cols] = out[0:count]
                xsend[at, :, cols] = out[count : 2 * count].reshape(PEERS, CAP, TILE).astype(jnp.bfloat16)
                return 0

            lax.fori_loop(0, width // TILE, project, 0)
            cross(c, xsend, xret, b_send, b_recv).start()

        @pl.when(step >= 2)
        def give_back():
            c = step - 2
            cross(c, xsend, xret, b_send, b_recv).wait_recv()
            at = pl.ds(c * PEERS, PEERS)
            total = kept[c % 2].reshape(PEERS, CAP, width) + xret[at].astype(jnp.float32)
            fin[at] = total.astype(jnp.bfloat16)
            for half in range(2):
                dz = step_along_z(c, half)

                def send(r, _, dz=dz, half=half):
                    k = c * PEERS + half * PLANE + r
                    other = peer_at(z, y, core, dz, r, -1)

                    @pl.when(k != SELF)
                    def away():
                        pltpu.make_async_remote_copy(
                            src_ref=fin.at[k], dst_ref=ret.at[sp],
                            send_sem=r_send.at[k], recv_sem=r_recv.at[k],
                            device_id=(other, tp), device_id_type=MESH,
                        ).start()

                    @pl.when(k == SELF)
                    def here():
                        pltpu.make_async_copy(fin.at[k], ret.at[sp], r_recv.at[k]).start()

                    return 0

                lax.fori_loop(0, PLANE, send, 0)

        return 0

    lax.fori_loop(0, GROUPS + 2, stage, 0)

    def finish(k, _):
        wait_for(ret.at[k], r_recv.at[k])

        @pl.when(k != SELF)
        def away():
            wait_for(recv.at[k], d_send.at[k])
            wait_for(fin.at[k], r_send.at[k])

        return 0

    lax.fori_loop(0, Z * PLANE, finish, 0)
    for c in range(GROUPS):
        cross(c, recv, xrecv, x_send, x_recv).wait_send()
        cross(c, xsend, xret, b_send, b_recv).wait_send()
    for copy in [halo_copy, *swaps, *stat_copies, *far_copies, *near_copies[0], *near_copies[1]]:
        copy.wait_send()

    def gather_rows(n, _):
        cols = pl.ds(pl.multiple_of(n * TILE, TILE), TILE)
        rows = ret[:, :, cols].astype(F32).reshape(experts * CAP, TILE).astype(BF16)
        both = jnp.dot(share[...], rows, preferred_element_type=F32)
        half = n // (half_width // TILE)
        to = pl.ds(pl.multiple_of(n * TILE - half * half_width, TILE), TILE)
        acc[half, :, to] = both[0:BLOCK] + both[BLOCK : 2 * BLOCK] + hidden[:, cols].astype(F32)
        return 0

    lax.fori_loop(0, width // TILE, gather_rows, 0)

    def last_norm(i, _):
        at = pl.ds(pl.multiple_of(i * strip, strip), strip)
        total = jnp.concatenate([acc[0, at], acc[1, at]], axis=1)
        out[at] = normalize(total, out_gain[...]).astype(BF16)
        return 0

    lax.fori_loop(0, BLOCK // strip, last_norm, 0)


def shards(
    glu_value,
    glu_gate,
    conv_kernel,
    norm_gain,
    mix_weight,
    residual,
    resid_gain,
    expert_ids,
    route_weight,
    w_gate,
    w_up,
    w_down,
    out_gain,
):
    width = residual.shape[1]
    units = w_down.shape[1]
    channels = glu_value.shape[1]
    groups = channels // LANES
    experts = N_SP
    count = PEERS * CAP
    dma = pltpu.SemaphoreType.DMA
    vmem, hbm = pl.BlockSpec(memory_space=pltpu.VMEM), pl.BlockSpec(memory_space=pl.ANY)
    moved = pltpu.VMEM((experts, CAP, width), BF16)
    return pl.pallas_call(
        layer_kernel,
        out_shape=jax.ShapeDtypeStruct((BLOCK, width), BF16),
        in_specs=[vmem] * 9 + [hbm] * 4,
        out_specs=vmem,
        scratch_shapes=[
            pltpu.VMEM((groups, ROWS + HALO, LANES), F32),
            pltpu.VMEM((groups, HALO, LANES), BF16),
            pltpu.VMEM((groups, HALO, LANES), BF16),
            pltpu.VMEM((groups, ROWS, LANES), F32),
            pltpu.VMEM((ROWS, LANES), F32),
            pltpu.VMEM((LANES, ROWS), F32),
            pltpu.VMEM((8, ROWS), F32),
            pltpu.VMEM((N_TP - 1, 8, ROWS), F32),
            pltpu.VMEM((ROWS, channels), BF16),
            pltpu.VMEM((channels, width), BF16),
            pltpu.VMEM((2, BLOCK, width // 2), BF16),
            pltpu.VMEM((2, BLOCK, width // 2), BF16),
            pltpu.VMEM((2, 2, BLOCK, width // 2), BF16),
            pltpu.VMEM((2, 2, BLOCK, width // 2), BF16),
            pltpu.VMEM((2, BLOCK, width // 2), F32),
            pltpu.VMEM((BLOCK, width), BF16),
            pltpu.VMEM((experts * CAP, BLOCK), BF16),
            pltpu.VMEM((2 * BLOCK, experts * CAP), BF16),
            moved,
            moved,
            pltpu.VMEM((2, width, units), BF16),
            pltpu.VMEM((2, width, units), BF16),
            pltpu.VMEM((2 * units, width), BF16),
            moved,
            moved,
            pltpu.VMEM((2 * count, width), BF16),
            pltpu.VMEM((2 * count, 2 * units), BF16),
            pltpu.VMEM((2, count, width), F32),
            moved,
            moved,
            moved,
            dma((experts,)), dma((experts,)),
            dma((GROUPS,)), dma((GROUPS,)),
            dma((GROUPS,)), dma((GROUPS,)),
            dma((experts,)), dma((experts,)),
            dma((5,)), dma((5,)), dma((4,)),
            dma((2,)), dma((3,)), dma((3,)),
            dma((2,)), dma((2,)), dma((4,)), dma((4,)),
        ],
        compiler_params=pltpu.CompilerParams(
            collective_id=0, has_side_effects=True, vmem_limit_bytes=60 * 2**20
        ),
        name="layer",
    )(
        glu_value, glu_gate, conv_kernel, norm_gain[None], residual, resid_gain[None], out_gain[None],
        expert_ids.T, route_weight.T, mix_weight, w_gate, w_up, w_down,
    )


def solution(mesh):
    in_specs = (
        P("sp", "tp"),
        P("sp", "tp"),
        P(None, "tp"),
        P("tp"),
        P("tp", None),
        P(("sp", "tp"), None),
        P(),
        P(("sp", "tp"), None),
        P(("sp", "tp"), None),
        P("sp", None, "tp"),
        P("sp", None, "tp"),
        P("sp", "tp", None),
        P(),
    )
    out_specs = P(("sp", "tp"), None)
    return jax.shard_map(shards, mesh=mesh, in_specs=in_specs, out_specs=out_specs, check_vma=False)
```

```python
import jax
import jax.numpy as jnp
from jax import lax
from jax.experimental import pallas as pl
from jax.experimental.pallas import tpu as pltpu
from jax.sharding import PartitionSpec as P

DC = 2048
EPSILON = 1e-05
LIMIT = 7.0
SLOPE = 1.702
Z, Y, CORES, N_TP = 8, 4, 2, 4
PLANE = Y * CORES
N_SP = Z * PLANE
BANDS = 4
GROUPS = 2 * BANDS
AHEAD = 3
SIDE = PLANE // 2
PEERS = 2 * SIDE
SELF_GROUP = 2
SELF = SELF_GROUP * PEERS + SIDE
CAP = 8
TILE = 256
LANES = 128
TAPS = 31
HALO = 32
ROWS = 512
BLOCK = 128
STRIPE = 64
MESH = pl.DeviceIdType.MESH
F32, BF16 = jnp.float32, jnp.bfloat16


def normalize(values, gain_vector):
    centre = jnp.mean(values, axis=-1, keepdims=True)
    spread = jnp.mean(jnp.square(values - centre), axis=-1, keepdims=True)
    return (values - centre) * lax.rsqrt(spread + EPSILON) * gain_vector


def position():
    sp, tp = lax.axis_index("sp"), lax.axis_index("tp")
    z, y, core = sp // PLANE, (sp // CORES) % Y, sp % CORES
    near, far = tp + 1 - 2 * (tp % 2), 3 - tp
    weight_partner = near * (1 - core) + far * core
    row_partner = near * core + far * (1 - core)
    return sp, tp, z, y, core, weight_partner, row_partner


def step_along_z(band, half):
    distance = 3 + band - 3 * (band // 2) - 2 * (band // 3)
    return distance if half == 0 else (Z - distance) * (1 - distance // 4)


def peer_at(z, y, core, dz, r, sign):
    return ((z + sign * dz + Z) % Z) * PLANE + ((y + sign * (r // 2) + Y) % Y) * CORES + (core + r % 2) % CORES


def wait_for(ref, sem):
    pltpu.make_async_copy(ref, ref, sem).wait()


def layer_kernel(
    value_h, gate_h, taps_h, norm_gain_h, residual_h, resid_gain_h, out_gain_h, ids_h, weights_h, mix_weight, w_gate, w_up, w_down,
    out,
    value, gate, taps, norm_gain, residual, resid_gain, out_gain, ids, weights, total_v, ext, halo_send, halo_recv, conv_v, stat_cols, stat_rows, stats_send, stats_recv, mix_in, mix_v,
    a_send_v, a_recv_v, b_send_v, b_recv_v, acc, hidden, held, share, slots, ret,
    gate_v, up_v, down_v, recv, xrecv, rows_v, act_v, kept, xsend, xret, fin,
    d_send, d_recv, x_send, x_recv, b_send, b_recv, r_send, r_recv, w_send, w_recv, l_sem,
    h_sem, s_send, s_recv, ra_send, ra_recv, rb_send, rb_recv,
):
    sp, tp, z, y, core, weight_partner, row_partner = position()
    barrier = pltpu.get_barrier_semaphore()

    def greet(i, _):
        other = lax.rem(sp + i, N_SP)
        pl.semaphore_signal(barrier, inc=1, device_id=(other, tp), device_id_type=MESH)
        return 0

    lax.fori_loop(1, N_SP, greet, 0)
    for i in range(1, N_TP):
        pl.semaphore_signal(barrier, inc=1, device_id=(sp, (tp + i) % N_TP), device_id_type=MESH)
    width = w_down.shape[2]
    half_units = w_down.shape[1]
    channels = value.shape[1]
    first_loads = [
        pltpu.make_async_copy(src, dst, l_sem.at[4 + i])
        for i, (src, dst) in enumerate([
            (value_h, value), (gate_h, gate), (taps_h, taps), (norm_gain_h, norm_gain),
            (residual_h, residual), (resid_gain_h, resid_gain), (out_gain_h, out_gain), (ids_h, ids), (weights_h, weights),
        ])
    ]
    loads = [
        pltpu.make_async_copy(mix_weight, mix_v, l_sem.at[3]),
        pltpu.make_async_copy(w_gate.at[0], gate_v.at[0], l_sem.at[0]),
        pltpu.make_async_copy(w_up.at[0], up_v.at[0], l_sem.at[1]),
        pltpu.make_async_copy(w_down.at[0], down_v.at[0:half_units], l_sem.at[2]),
    ]
    for load in first_loads + loads:
        load.start()
    for load in first_loads[:2]:
        load.wait()

    lane_groups = channels // LANES

    def gated(rows, cols):
        product = value[rows, cols].astype(F32) * jax.nn.sigmoid(gate[rows, cols].astype(F32))
        return product.astype(BF16)

    for g in range(lane_groups):
        halo_send[g] = gated(pl.ds(ROWS - HALO, HALO), pl.ds(g * LANES, LANES))

    def gate_rows(i, _):
        for g in range(lane_groups):
            at = pl.ds(pl.multiple_of(i * STRIPE, STRIPE), STRIPE)
            to = pl.ds(pl.multiple_of(i * STRIPE + HALO, HALO), STRIPE)
            ext[g, to] = gated(at, pl.ds(g * LANES, LANES)).astype(F32)
        return 0

    lax.fori_loop(0, ROWS // STRIPE, gate_rows, 0)
    for load in first_loads[2:]:
        load.wait()
    pl.semaphore_wait(barrier, N_SP - 1 + N_TP - 1)
    halo_copy = pltpu.make_async_remote_copy(
        src_ref=halo_send, dst_ref=halo_recv, send_sem=h_sem.at[0], recv_sem=h_sem.at[1],
        device_id=(lax.rem(sp + 1, N_SP), tp), device_id_type=MESH,
    )
    halo_copy.start()

    def swap(i, src, dst):
        return pltpu.make_async_remote_copy(
            src_ref=src, dst_ref=dst, send_sem=w_send.at[i], recv_sem=w_recv.at[i],
            device_id=(sp, weight_partner), device_id_type=MESH,
        )

    def rows_of(ref, first, last):
        return ref.at[pl.ds(first, last - first)]

    cuts = (0, 768, 1536, 2048)
    swaps = [
        swap(i, w_gate.at[0, pl.ds(f, l - f)], gate_v.at[1, pl.ds(f, l - f)])
        for i, (f, l) in enumerate(zip(cuts, cuts[1:]))
    ] + [
        swap(3, w_up.at[0], up_v.at[1]),
        swap(4, w_down.at[0], down_v.at[half_units : 2 * half_units]),
    ]
    swaps[0].start()

    lane = lax.broadcasted_iota(jnp.int32, (STRIPE, LANES), 1)

    def convolve(i):
        first = pl.multiple_of(i * STRIPE, STRIPE)
        total, square = jnp.zeros((STRIPE, LANES), F32), jnp.zeros((STRIPE, LANES), F32)
        for g in range(lane_groups):
            sums = jnp.zeros((STRIPE, LANES), F32)
            for k in range(TAPS):
                tap = taps[k : k + 1, g * LANES : (g + 1) * LANES]
                sums = sums + tap * ext[g, pl.ds(first + (HALO - TAPS + 1 + k), STRIPE)]
            conv_v[g, pl.ds(first, STRIPE)] = sums
            total, square = total + sums, square + sums * sums
        total = jnp.sum(total, axis=1, keepdims=True)
        square = jnp.sum(square, axis=1, keepdims=True)
        stat_cols[pl.ds(first, STRIPE)] = jnp.where(lane == 0, total, jnp.where(lane == 1, square, 0.0))

    def convolve_step(i, _):
        convolve(i)
        return 0

    lax.fori_loop(1, ROWS // STRIPE, convolve_step, 0)
    halo_copy.wait_recv()
    for g in range(lane_groups):
        ext[g, 0:HALO] = jnp.where(sp > 0, halo_recv[g].astype(F32), 0.0)
    convolve(0)
    for i in range(ROWS // LANES):
        at = slice(i * LANES, (i + 1) * LANES)
        stats_send[:, at] = jnp.transpose(stat_cols[at, :])[0:8]
    stat_copies = [
        pltpu.make_async_remote_copy(
            src_ref=stats_send, dst_ref=stats_recv.at[j - 1], send_sem=s_send.at[j - 1], recv_sem=s_recv.at[j - 1],
            device_id=(sp, (tp + j) % N_TP), device_id_type=MESH,
        )
        for j in (2, 1, 3)
    ]
    for c in stat_copies:
        c.start()
    swaps[1].start()

    experts = N_SP
    spot = lax.broadcasted_iota(jnp.int32, (experts, BLOCK), 0)
    one = [(spot == ids[j : j + 1, :]).astype(BF16) for j in range(2)]
    before = lax.broadcasted_iota(jnp.int32, (BLOCK, BLOCK), 0) < lax.broadcasted_iota(jnp.int32, (BLOCK, BLOCK), 1)
    earlier = jnp.dot(one[0] + one[1], before.astype(BF16), preferred_element_type=F32)
    place = lax.broadcasted_iota(jnp.int32, (experts * CAP, experts), 0) // CAP
    group = place // PEERS
    band, r = group // 2, (group % 2) * SIDE + place % SIDE
    step = jnp.where((place // SIDE) % 2 == 0, step_along_z(band, 0), step_along_z(band, 1))
    owner = peer_at(z, y, core, step, r, 1)
    spread_out = (owner == lax.broadcasted_iota(jnp.int32, (experts * CAP, experts), 1)).astype(BF16)
    rank = jnp.dot(spread_out, earlier.astype(BF16), preferred_element_type=F32)
    in_rank = rank == (lax.broadcasted_iota(jnp.int32, (experts * CAP, BLOCK), 0) % CAP).astype(F32)
    hits = [
        jnp.where(in_rank, jnp.dot(spread_out, o, preferred_element_type=F32), 0.0) for o in one
    ]
    held[...] = (hits[0] + hits[1]).astype(BF16)
    shares = hits[0] * weights[0:1, :] + hits[1] * weights[1:2, :]
    for i in range(experts * CAP // LANES):
        at = slice(i * LANES, (i + 1) * LANES)
        part = jnp.transpose(shares[at, :])
        high = part.astype(BF16)
        share[0:BLOCK, at] = high
        share[BLOCK : 2 * BLOCK, at] = (part - high.astype(F32)).astype(BF16)
    stat_rows[...] = jnp.zeros_like(stat_rows)

    for c in stat_copies:
        c.wait_recv()
    sums = stats_send[...] + stats_recv[0] + stats_recv[1] + stats_recv[2]
    centre = sums[0:1] / DC
    scale = lax.rsqrt(sums[1:2] / DC - centre * centre + EPSILON)
    stat_rows[0:1] = centre
    stat_rows[1:2] = scale

    loads[0].wait()

    def mix_rows(b):
        at = pl.ds(pl.multiple_of(b * BLOCK, BLOCK), BLOCK)
        columns = jnp.transpose(stat_rows[:, at])
        for g in range(lane_groups):
            lanes = slice(g * LANES, (g + 1) * LANES)
            v = (conv_v[g, at] - columns[:, 0:1]) * columns[:, 1:2] * norm_gain[:, lanes]
            mix_in[at, lanes] = (v / (1.0 + jnp.exp(-v))).astype(BF16)

    half_width = width // 2

    def project_rows(b, half, into):
        at = pl.ds(pl.multiple_of(b * BLOCK, BLOCK), BLOCK)

        def one_tile(n, _):
            col = pl.multiple_of(n * TILE, TILE)
            cols = pl.ds(pl.multiple_of(half * half_width + n * TILE, TILE), TILE)
            into(pl.ds(col, TILE), jnp.dot(mix_in[at, :], mix_v[:, cols], preferred_element_type=F32))
            return 0

        lax.fori_loop(0, half_width // TILE, one_tile, 0)

    def to_neighbour(src, dst, send_sem, recv_sem, side):
        return pltpu.make_async_remote_copy(
            src_ref=src, dst_ref=dst, send_sem=send_sem, recv_sem=recv_sem,
            device_id=(sp, (tp + (1 if side == 0 else N_TP - 1)) % N_TP), device_id_type=MESH,
        )

    far_copies = [
        to_neighbour(a_send_v.at[i], a_recv_v.at[i], ra_send.at[i], ra_recv.at[i], i) for i in range(2)
    ]
    near_copies = [
        [
            to_neighbour(
                b_send_v.at[i, h], b_recv_v.at[i, h], rb_send.at[2 * i + h], rb_recv.at[2 * i + h], i
            )
            for h in range(2)
        ]
        for i in range(2)
    ]
    far = (tp + 2) % N_TP
    sides = [(tp + 1) % N_TP, (tp + N_TP - 1) % N_TP]
    mix_rows(far)
    for i in range(2):

        def keep(cols, product, i=i):
            a_send_v[i, :, cols] = product.astype(BF16)

        project_rows(far, i, keep)
        far_copies[i].start()
    for i in range(2):
        mix_rows(sides[i])

        def keep(cols, product, i=i):
            b_send_v[i, 1 - i, :, cols] = product.astype(BF16)

        project_rows(sides[i], 1 - i, keep)
        near_copies[i][1 - i].start()
    for i in range(2):
        far_copies[i].wait_recv()

        def keep(cols, product, i=i):
            b_send_v[i, i, :, cols] = (product + a_recv_v[i, :, cols].astype(F32)).astype(BF16)

        project_rows(sides[i], i, keep)
        near_copies[i][i].start()
    for s in swaps[2:]:
        s.start()
    mix_rows(tp)
    for h in range(2):

        def keep(cols, product, h=h):
            acc[h, :, cols] = product

        project_rows(tp, h, keep)
    for i in range(2):
        near_copies[i][1 - i].wait_recv()
    for i in range(2):
        near_copies[i][i].wait_recv()

    strip = 16

    def norm_rows(i, _):
        at = pl.ds(pl.multiple_of(i * strip, strip), strip)
        halves = [
            acc[h, at] + b_recv_v[0, h, at].astype(F32) + b_recv_v[1, h, at].astype(F32) for h in range(2)
        ]
        total = jnp.concatenate(halves, axis=1) + residual[at].astype(F32)
        rows = normalize(total, resid_gain[...]).astype(BF16)
        hidden[at] = rows
        total_v[at] = rows.astype(F32)
        return 0

    lax.fori_loop(0, BLOCK // strip, norm_rows, 0, unroll=True)

    band_slots = 2 * PEERS * CAP

    def fill_slots(band):
        at = slice(band * band_slots, (band + 1) * band_slots)

        def one_tile(n, _):
            cols = pl.ds(pl.multiple_of(n * TILE, TILE), TILE)
            picked = jnp.dot(held[at, :], hidden[:, cols], preferred_element_type=F32)
            to = slice(band * 2 * PEERS, (band + 1) * 2 * PEERS)
            slots[to, :, cols] = picked.reshape(2 * PEERS, CAP, TILE).astype(BF16)
            return 0

        lax.fori_loop(0, width // TILE, one_tile, 0)

    for group in range(GROUPS):
        if group % 2 == 0:
            fill_slots(group // 2)
        if group == SELF_GROUP:
            pltpu.make_async_copy(slots.at[SELF], recv.at[SELF], d_recv.at[SELF]).start()
        for half in range(2):
            dz = step_along_z(group // 2, half)
            base = group * PEERS + half * SIDE

            def send(r, _, dz=dz, base=base, group=group):
                other = peer_at(z, y, core, dz, (group % 2) * SIDE + r, 1)
                pltpu.make_async_remote_copy(
                    src_ref=slots.at[base + r], dst_ref=recv.at[base + r],
                    send_sem=d_send.at[base + r], recv_sem=d_recv.at[base + r],
                    device_id=(other, tp), device_id_type=MESH,
                ).start()
                return 0

            lax.fori_loop(1 if base == SELF else 0, SIDE, send, 0)

    def cross(c, src, dst, send_sem, recv_sem):
        return pltpu.make_async_remote_copy(
            src_ref=src.at[pl.ds(c * PEERS, PEERS)], dst_ref=dst.at[pl.ds(c * PEERS, PEERS)],
            send_sem=send_sem.at[c], recv_sem=recv_sem.at[c],
            device_id=(sp, row_partner), device_id_type=MESH,
        )

    def cross_back(c, half):
        at, cols = pl.ds(c * PEERS, PEERS), pl.ds(half * half_width, half_width)
        return pltpu.make_async_remote_copy(
            src_ref=xsend.at[at, :, cols], dst_ref=xret.at[at, :, cols],
            send_sem=b_send.at[2 * c + half], recv_sem=b_recv.at[2 * c + half],
            device_id=(sp, row_partner), device_id_type=MESH,
        )

    count = PEERS * CAP

    def arrive(group):
        def one(r, _):
            wait_for(recv.at[group * PEERS + r], d_recv.at[group * PEERS + r])
            return 0

        lax.fori_loop(0, PEERS, one, 0)
        cross(group, recv, xrecv, x_send, x_recv).start()

    def compute(c):
        cross(c, recv, xrecv, x_send, x_recv).wait_recv()
        at = pl.ds(c * PEERS, PEERS)
        rows_v[0:count] = recv[at].astype(F32).reshape(count, width).astype(BF16)
        rows_v[count : 2 * count] = xrecv[at].astype(F32).reshape(count, width).astype(BF16)

        def activate(j, _):
            half, col = j // 2, pl.multiple_of((j % 2) * TILE, TILE)
            g = jnp.dot(rows_v[...], gate_v[half, :, pl.ds(col, TILE)], preferred_element_type=F32)
            u = jnp.dot(rows_v[...], up_v[half, :, pl.ds(col, TILE)], preferred_element_type=F32)
            g = jnp.minimum(g, LIMIT)
            u = jnp.clip(u, -LIMIT, LIMIT)
            act = (u + 1.0) * g * jax.nn.sigmoid(SLOPE * g)
            act_v[:, pl.ds(pl.multiple_of(j * TILE, TILE), TILE)] = act.astype(BF16)
            return 0

        lax.fori_loop(0, 2 * half_units // TILE, activate, 0)

        @pl.when(c == 0)
        def down_weights():
            swaps[-1].wait_recv()

        def project(n, _):
            cols = pl.ds(pl.multiple_of(n * TILE, TILE), TILE)
            result = jnp.dot(act_v[...], down_v[:, cols], preferred_element_type=F32)
            kept[c % 2, :, cols] = result[0:count]
            xsend[at, :, cols] = result[count : 2 * count].reshape(PEERS, CAP, TILE).astype(BF16)
            return 0

        tiles = half_width // TILE
        for half in range(2):
            lax.fori_loop(half * tiles, (half + 1) * tiles, project, 0)
            cross_back(c, half).start()

    def give_back(c):
        at = pl.ds(c * PEERS, PEERS)
        for half in range(2):
            cross_back(c, half).wait_recv()
        total = kept[c % 2].reshape(PEERS, CAP, width) + xret[at].astype(F32)
        fin[at] = total.astype(BF16)
        for half in range(2):
            dz = step_along_z(c // 2, half)

            def send(r, _, dz=dz, half=half):
                k = c * PEERS + half * SIDE + r
                other = peer_at(z, y, core, dz, (c % 2) * SIDE + r, -1)

                @pl.when(k != SELF)
                def away():
                    pltpu.make_async_remote_copy(
                        src_ref=fin.at[k], dst_ref=ret.at[k],
                        send_sem=r_send.at[k], recv_sem=r_recv.at[k],
                        device_id=(other, tp), device_id_type=MESH,
                    ).start()

                @pl.when(k == SELF)
                def here():
                    pltpu.make_async_copy(fin.at[k], ret.at[k], r_recv.at[k]).start()

                return 0

            lax.fori_loop(0, SIDE, send, 0)

    arrive(0)
    for load in loads[1:]:
        load.wait()
    for s in swaps[:-1]:
        s.wait_recv()

    def stage(c, _):
        @pl.when(c == 1)
        def early():
            give_back(0)

        compute(c)

        @pl.when(c == 0)
        def next_rows():
            for group in range(1, AHEAD):
                arrive(group)

        @pl.when(c < GROUPS - AHEAD)
        def later_rows():
            arrive(c + AHEAD)

        @pl.when(c >= 2)
        def late():
            give_back(c - 1)

        return 0

    def gather_band(band, _):
        def one(r, _):
            wait_for(ret.at[band * 2 * PEERS + r], r_recv.at[band * 2 * PEERS + r])
            return 0

        lax.fori_loop(0, 2 * PEERS, one, 0)
        own = share[:, pl.ds(pl.multiple_of(band * band_slots, band_slots), band_slots)]

        def one_tile(n, _):
            cols = pl.ds(pl.multiple_of(n * TILE, TILE), TILE)
            rows = ret[pl.ds(band * 2 * PEERS, 2 * PEERS), :, cols].astype(F32).reshape(band_slots, TILE).astype(BF16)
            both = jnp.dot(own, rows, preferred_element_type=F32)
            total_v[:, cols] += both[0:BLOCK] + both[BLOCK : 2 * BLOCK]
            return 0

        lax.fori_loop(0, width // TILE, one_tile, 0)
        return 0

    lax.fori_loop(0, GROUPS, stage, 0)
    lax.fori_loop(0, BANDS - 2, gather_band, 0)
    give_back(GROUPS - 1)

    def sent(k, _):
        @pl.when(k != SELF)
        def away():
            wait_for(recv.at[k], d_send.at[k])
            wait_for(fin.at[k], r_send.at[k])

        return 0

    lax.fori_loop(BANDS - 2, BANDS - 1, gather_band, 0)
    lax.fori_loop(0, N_SP, sent, 0)
    for c in range(GROUPS):
        cross(c, recv, xrecv, x_send, x_recv).wait_send()
        for half in range(2):
            cross_back(c, half).wait_send()
    for copy in [halo_copy, *swaps, *stat_copies, *far_copies, *near_copies[0], *near_copies[1]]:
        copy.wait_send()
    gather_band(BANDS - 1, 0)

    def last_norm(i, _):
        at = pl.ds(pl.multiple_of(i * strip, strip), strip)
        out[at] = normalize(total_v[at], out_gain[...]).astype(BF16)
        return 0

    lax.fori_loop(0, BLOCK // strip, last_norm, 0, unroll=True)


def shards(
    glu_value,
    glu_gate,
    conv_kernel,
    norm_gain,
    mix_weight,
    residual,
    resid_gain,
    expert_ids,
    route_weight,
    w_gate,
    w_up,
    w_down,
    out_gain,
):
    width = residual.shape[1]
    units = w_down.shape[1]
    channels = glu_value.shape[1]
    groups = channels // LANES
    experts = N_SP
    count = PEERS * CAP
    dma = pltpu.SemaphoreType.DMA
    vmem, hbm = pl.BlockSpec(memory_space=pltpu.VMEM), pl.BlockSpec(memory_space=pltpu.MemorySpace.HBM)
    moved = pltpu.VMEM((experts, CAP, width), BF16)
    return pl.pallas_call(
        layer_kernel,
        out_shape=jax.ShapeDtypeStruct((BLOCK, width), BF16),
        in_specs=[hbm] * 13,
        out_specs=vmem,
        scratch_shapes=[
            pltpu.VMEM(glu_value.shape, BF16),
            pltpu.VMEM(glu_gate.shape, BF16),
            pltpu.VMEM(conv_kernel.shape, F32),
            pltpu.VMEM((1, channels), F32),
            pltpu.VMEM(residual.shape, BF16),
            pltpu.VMEM((1, width), F32),
            pltpu.VMEM((1, width), F32),
            pltpu.VMEM((2, BLOCK), jnp.int32),
            pltpu.VMEM((2, BLOCK), F32),
            pltpu.VMEM((BLOCK, width), F32),
            pltpu.VMEM((groups, ROWS + HALO, LANES), F32),
            pltpu.VMEM((groups, HALO, LANES), BF16),
            pltpu.VMEM((groups, HALO, LANES), BF16),
            pltpu.VMEM((groups, ROWS, LANES), F32),
            pltpu.VMEM((ROWS, LANES), F32),
            pltpu.VMEM((LANES, ROWS), F32),
            pltpu.VMEM((8, ROWS), F32),
            pltpu.VMEM((N_TP - 1, 8, ROWS), F32),
            pltpu.VMEM((ROWS, channels), BF16),
            pltpu.VMEM((channels, width), BF16),
            pltpu.VMEM((2, BLOCK, width // 2), BF16),
            pltpu.VMEM((2, BLOCK, width // 2), BF16),
            pltpu.VMEM((2, 2, BLOCK, width // 2), BF16),
            pltpu.VMEM((2, 2, BLOCK, width // 2), BF16),
            pltpu.VMEM((2, BLOCK, width // 2), F32),
            pltpu.VMEM((BLOCK, width), BF16),
            pltpu.VMEM((experts * CAP, BLOCK), BF16),
            pltpu.VMEM((2 * BLOCK, experts * CAP), BF16),
            moved,
            moved,
            pltpu.VMEM((2, width, units), BF16),
            pltpu.VMEM((2, width, units), BF16),
            pltpu.VMEM((2 * units, width), BF16),
            moved,
            moved,
            pltpu.VMEM((2 * count, width), BF16),
            pltpu.VMEM((2 * count, 2 * units), BF16),
            pltpu.VMEM((2, count, width), F32),
            moved,
            moved,
            moved,
            dma((experts,)), dma((experts,)),
            dma((GROUPS,)), dma((GROUPS,)),
            dma((2 * GROUPS,)), dma((2 * GROUPS,)),
            dma((experts,)), dma((experts,)),
            dma((5,)), dma((5,)), dma((13,)),
            dma((2,)), dma((3,)), dma((3,)),
            dma((2,)), dma((2,)), dma((4,)), dma((4,)),
        ],
        compiler_params=pltpu.CompilerParams(
            collective_id=0, has_side_effects=True, vmem_limit_bytes=60 * 2**20
        ),
        name="layer",
    )(
        glu_value, glu_gate, conv_kernel, norm_gain[None], residual, resid_gain[None], out_gain[None],
        expert_ids.T, route_weight.T, mix_weight, w_gate, w_up, w_down,
    )


def solution(mesh):
    in_specs = (
        P("sp", "tp"),
        P("sp", "tp"),
        P(None, "tp"),
        P("tp"),
        P("tp", None),
        P(("sp", "tp"), None),
        P(),
        P(("sp", "tp"), None),
        P(("sp", "tp"), None),
        P("sp", None, "tp"),
        P("sp", None, "tp"),
        P("sp", "tp", None),
        P(),
    )
    out_specs = P(("sp", "tp"), None)
    return jax.shard_map(shards, mesh=mesh, in_specs=in_specs, out_specs=out_specs, check_vma=False)
```

```python
import jax
import jax.numpy as jnp
from jax import lax
from jax.experimental import pallas as pl
from jax.experimental.pallas import tpu as pltpu
from jax.sharding import PartitionSpec as P

DC = 2048
EPSILON = 1e-05
LIMIT = 7.0
SLOPE = 1.702
Z, Y, CORES, N_TP = 8, 4, 2, 4
PLANE = Y * CORES
N_SP = Z * PLANE
BANDS = 4
GROUPS = 2 * BANDS
FIRST = 2
SIDE = PLANE // 2
PEERS = 2 * SIDE
SELF_GROUP = 3
SELF = SELF_GROUP * PEERS + SIDE
CAP = 8
TILE = 256
LANES = 128
TAPS = 31
HALO = 32
ROWS = 512
BLOCK = 128
STRIPE = 64
MESH = pl.DeviceIdType.MESH
F32, BF16 = jnp.float32, jnp.bfloat16


def normalize(values, gain_vector):
    centre = jnp.mean(values, axis=-1, keepdims=True)
    spread = jnp.mean(jnp.square(values - centre), axis=-1, keepdims=True)
    return (values - centre) * lax.rsqrt(spread + EPSILON) * gain_vector


def position():
    sp, tp = lax.axis_index("sp"), lax.axis_index("tp")
    z, y, core = sp // PLANE, (sp // CORES) % Y, sp % CORES
    near, far = tp + 1 - 2 * (tp % 2), 3 - tp
    weight_partner = near * (1 - core) + far * core
    row_partner = near * core + far * (1 - core)
    return sp, tp, z, y, core, weight_partner, row_partner


def step_along_z(band, half):
    distance = 3 + band - 3 * (band // 2) - 2 * (band // 3)
    return distance if half == 0 else (Z - distance) * (1 - distance // 4)


def peer_at(z, y, core, dz, r, sign):
    return ((z + sign * dz + Z) % Z) * PLANE + ((y + sign * (r // 2) + Y) % Y) * CORES + (core + r % 2) % CORES


def wait_for(ref, sem):
    pltpu.make_async_copy(ref, ref, sem).wait()


def layer_kernel(
    value_h, gate_h, taps_h, norm_gain_h, residual_h, resid_gain_h, out_gain_h, ids_h, weights_h, mix_weight, w_gate, w_up, w_down,
    out,
    value, gate, taps, norm_gain, residual, resid_gain, out_gain, ids, weights, total_v, ext, halo_send, halo_recv, conv_v, stat_cols, stat_rows, stats_send, stats_recv, mix_in, mix_v,
    a_send_v, a_recv_v, b_send_v, b_recv_v, acc, hidden, held, share, slots, ret,
    gate_v, up_v, down_v, recv, xrecv, rows_v, act_v, kept, xsend, xret, fin,
    d_send, d_recv, x_send, x_recv, b_send, b_recv, r_send, r_recv, w_send, w_recv, l_sem,
    word, h_sem, s_send, s_recv, ra_send, ra_recv, rb_send, rb_recv,
):
    sp, tp, z, y, core, weight_partner, row_partner = position()
    barrier = pltpu.get_barrier_semaphore()

    along_z = [((z + d) % Z) * PLANE + sp % PLANE for d in (1, Z - 1)]
    along_y = [z * PLANE + ((y + d) % Y) * CORES + core for d in (1, Y - 1)]
    along_sp = [(sp + d) % N_SP for d in (1, N_SP - 1)]
    for other in along_sp + along_z + along_y:
        pl.semaphore_signal(barrier, inc=1, device_id=(other, tp), device_id_type=MESH)
    for i in range(1, N_TP):
        pl.semaphore_signal(barrier, inc=1, device_id=(sp, (tp + i) % N_TP), device_id_type=MESH)
    rounds = [along_z] * 3 + [along_y] * 2 + [[z * PLANE + y * CORES + 1 - core]]

    def tell(i):
        for other in rounds[i]:
            pl.semaphore_signal(word.at[i], inc=1, device_id=(other, tp), device_id_type=MESH)

    def hear(i):
        pl.semaphore_wait(word.at[i], len(rounds[i]))
        if i + 1 < len(rounds):
            tell(i + 1)

    width = w_down.shape[2]
    half_units = w_down.shape[1]
    half_width = width // 2
    channels = value.shape[1]
    first_loads = [
        pltpu.make_async_copy(src, dst, l_sem.at[4 + i])
        for i, (src, dst) in enumerate([
            (value_h, value), (gate_h, gate), (taps_h, taps), (norm_gain_h, norm_gain),
            (residual_h, residual), (resid_gain_h, resid_gain), (out_gain_h, out_gain), (ids_h, ids), (weights_h, weights),
        ])
    ]
    loads = [
        pltpu.make_async_copy(mix_weight, mix_v, l_sem.at[3]),
        pltpu.make_async_copy(w_gate.at[0], gate_v.at[0], l_sem.at[0]),
        pltpu.make_async_copy(w_up.at[0], up_v.at[0], l_sem.at[1]),
        pltpu.make_async_copy(w_down.at[0], down_v.at[0:half_units], l_sem.at[2]),
    ]
    for load in first_loads + loads:
        load.start()
    for load in first_loads[:2]:
        load.wait()

    lane_groups = channels // LANES

    def gated(rows, cols):
        product = value[rows, cols].astype(F32) * jax.nn.sigmoid(gate[rows, cols].astype(F32))
        return product.astype(BF16)

    for g in range(lane_groups):
        halo_send[g] = gated(pl.ds(ROWS - HALO, HALO), pl.ds(g * LANES, LANES))

    def gate_rows(i, _):
        for g in range(lane_groups):
            at = pl.ds(pl.multiple_of(i * STRIPE, STRIPE), STRIPE)
            to = pl.ds(pl.multiple_of(i * STRIPE + HALO, HALO), STRIPE)
            ext[g, to] = gated(at, pl.ds(g * LANES, LANES)).astype(F32)
        return 0

    lax.fori_loop(0, ROWS // STRIPE, gate_rows, 0)
    for load in first_loads[2:]:
        load.wait()
    pl.semaphore_wait(barrier, 6 + N_TP - 1)
    tell(0)
    halo_copy = pltpu.make_async_remote_copy(
        src_ref=halo_send, dst_ref=halo_recv, send_sem=h_sem.at[0], recv_sem=h_sem.at[1],
        device_id=(lax.rem(sp + 1, N_SP), tp), device_id_type=MESH,
    )
    halo_copy.start()

    def swap(i, src, dst):
        return pltpu.make_async_remote_copy(
            src_ref=src, dst_ref=dst, send_sem=w_send.at[i], recv_sem=w_recv.at[i],
            device_id=(sp, weight_partner), device_id_type=MESH,
        )

    def rows_of(ref, first, last):
        return ref.at[pl.ds(first, last - first)]

    cuts = (0, 768, 1536, 2048)
    swaps = [
        swap(i, w_gate.at[0, pl.ds(f, l - f)], gate_v.at[1, pl.ds(f, l - f)])
        for i, (f, l) in enumerate(zip(cuts, cuts[1:]))
    ] + [
        swap(3, w_up.at[0], up_v.at[1]),
    ] + [
        swap(
            4 + h, w_down.at[0, :, pl.ds(h * half_width, half_width)],
            down_v.at[pl.ds(half_units, half_units), pl.ds(h * half_width, half_width)],
        )
        for h in range(2)
    ]
    swaps[0].start()

    lane = lax.broadcasted_iota(jnp.int32, (STRIPE, LANES), 1)

    def convolve(i):
        first = pl.multiple_of(i * STRIPE, STRIPE)
        total, square = jnp.zeros((STRIPE, LANES), F32), jnp.zeros((STRIPE, LANES), F32)
        for g in range(lane_groups):
            sums = jnp.zeros((STRIPE, LANES), F32)
            for k in range(TAPS):
                tap = taps[k : k + 1, g * LANES : (g + 1) * LANES]
                sums = sums + tap * ext[g, pl.ds(first + (HALO - TAPS + 1 + k), STRIPE)]
            conv_v[g, pl.ds(first, STRIPE)] = sums
            total, square = total + sums, square + sums * sums
        total = jnp.sum(total, axis=1, keepdims=True)
        square = jnp.sum(square, axis=1, keepdims=True)
        stat_cols[pl.ds(first, STRIPE)] = jnp.where(lane == 0, total, jnp.where(lane == 1, square, 0.0))

    def convolve_step(i, _):
        convolve(i)
        return 0

    lax.fori_loop(1, ROWS // STRIPE, convolve_step, 0)
    hear(0)
    halo_copy.wait_recv()
    for g in range(lane_groups):
        ext[g, 0:HALO] = jnp.where(sp > 0, halo_recv[g].astype(F32), 0.0)
    convolve(0)
    for i in range(ROWS // LANES):
        at = slice(i * LANES, (i + 1) * LANES)
        stats_send[:, at] = jnp.transpose(stat_cols[at, :])[0:8]
    stat_copies = [
        pltpu.make_async_remote_copy(
            src_ref=stats_send, dst_ref=stats_recv.at[j - 1], send_sem=s_send.at[j - 1], recv_sem=s_recv.at[j - 1],
            device_id=(sp, (tp + j) % N_TP), device_id_type=MESH,
        )
        for j in (2, 1, 3)
    ]
    for c in stat_copies:
        c.start()
    swaps[1].start()

    hear(1)

    experts = N_SP
    spot = lax.broadcasted_iota(jnp.int32, (experts, BLOCK), 0)
    one = [(spot == ids[j : j + 1, :]).astype(BF16) for j in range(2)]
    before = lax.broadcasted_iota(jnp.int32, (BLOCK, BLOCK), 0) < lax.broadcasted_iota(jnp.int32, (BLOCK, BLOCK), 1)
    earlier = jnp.dot(one[0] + one[1], before.astype(BF16), preferred_element_type=F32)
    place = lax.broadcasted_iota(jnp.int32, (experts * CAP, experts), 0) // CAP
    group = place // PEERS
    band, r = group // 2, (1 - group % 2) * SIDE + place % SIDE
    step = jnp.where((place // SIDE) % 2 == 0, step_along_z(band, 0), step_along_z(band, 1))
    owner = peer_at(z, y, core, step, r, 1)
    spread_out = (owner == lax.broadcasted_iota(jnp.int32, (experts * CAP, experts), 1)).astype(BF16)
    rank = jnp.dot(spread_out, earlier.astype(BF16), preferred_element_type=F32)
    in_rank = rank == (lax.broadcasted_iota(jnp.int32, (experts * CAP, BLOCK), 0) % CAP).astype(F32)
    hits = [
        jnp.where(in_rank, jnp.dot(spread_out, o, preferred_element_type=F32), 0.0) for o in one
    ]
    held[...] = (hits[0] + hits[1]).astype(BF16)
    shares = hits[0] * weights[0:1, :] + hits[1] * weights[1:2, :]
    for i in range(experts * CAP // LANES):
        at = slice(i * LANES, (i + 1) * LANES)
        part = jnp.transpose(shares[at, :])
        high = part.astype(BF16)
        share[0:BLOCK, at] = high
        share[BLOCK : 2 * BLOCK, at] = (part - high.astype(F32)).astype(BF16)
    stat_rows[...] = jnp.zeros_like(stat_rows)
    hear(2)

    for c in stat_copies:
        c.wait_recv()
    sums = stats_send[...] + stats_recv[0] + stats_recv[1] + stats_recv[2]
    centre = sums[0:1] / DC
    scale = lax.rsqrt(sums[1:2] / DC - centre * centre + EPSILON)
    stat_rows[0:1] = centre
    stat_rows[1:2] = scale

    loads[0].wait()

    def mix_rows(b):
        at = pl.ds(pl.multiple_of(b * BLOCK, BLOCK), BLOCK)
        columns = jnp.transpose(stat_rows[:, at])
        for g in range(lane_groups):
            lanes = slice(g * LANES, (g + 1) * LANES)
            v = (conv_v[g, at] - columns[:, 0:1]) * columns[:, 1:2] * norm_gain[:, lanes]
            mix_in[at, lanes] = (v / (1.0 + jnp.exp(-v))).astype(BF16)

    def project_rows(b, half, into):
        at = pl.ds(pl.multiple_of(b * BLOCK, BLOCK), BLOCK)

        def one_tile(n, _):
            col = pl.multiple_of(n * TILE, TILE)
            cols = pl.ds(pl.multiple_of(half * half_width + n * TILE, TILE), TILE)
            into(pl.ds(col, TILE), jnp.dot(mix_in[at, :], mix_v[:, cols], preferred_element_type=F32))
            return 0

        lax.fori_loop(0, half_width // TILE, one_tile, 0)

    def to_neighbour(src, dst, send_sem, recv_sem, side):
        return pltpu.make_async_remote_copy(
            src_ref=src, dst_ref=dst, send_sem=send_sem, recv_sem=recv_sem,
            device_id=(sp, (tp + (1 if side == 0 else N_TP - 1)) % N_TP), device_id_type=MESH,
        )

    far_copies = [
        to_neighbour(a_send_v.at[i], a_recv_v.at[i], ra_send.at[i], ra_recv.at[i], i) for i in range(2)
    ]
    near_copies = [
        [
            to_neighbour(
                b_send_v.at[i, h], b_recv_v.at[i, h], rb_send.at[2 * i + h], rb_recv.at[2 * i + h], i
            )
            for h in range(2)
        ]
        for i in range(2)
    ]
    hear(3)
    far = (tp + 2) % N_TP
    sides = [(tp + 1) % N_TP, (tp + N_TP - 1) % N_TP]
    mix_rows(far)
    for i in range(2):

        def keep(cols, product, i=i):
            a_send_v[i, :, cols] = product.astype(BF16)

        project_rows(far, i, keep)
        far_copies[i].start()
    for i in range(2):
        mix_rows(sides[i])

        def keep(cols, product, i=i):
            b_send_v[i, 1 - i, :, cols] = product.astype(BF16)

        project_rows(sides[i], 1 - i, keep)
        near_copies[i][1 - i].start()
    for i in range(2):
        far_copies[i].wait_recv()

        def keep(cols, product, i=i):
            b_send_v[i, i, :, cols] = (product + a_recv_v[i, :, cols].astype(F32)).astype(BF16)

        project_rows(sides[i], i, keep)
        near_copies[i][i].start()
    for s in swaps[2:]:
        s.start()
    hear(4)
    mix_rows(tp)
    for h in range(2):

        def keep(cols, product, h=h):
            acc[h, :, cols] = product

        project_rows(tp, h, keep)
    for i in range(2):
        near_copies[i][1 - i].wait_recv()
    for i in range(2):
        near_copies[i][i].wait_recv()

    strip = 16

    def norm_rows(i, _):
        at = pl.ds(pl.multiple_of(i * strip, strip), strip)
        halves = [
            acc[h, at] + b_recv_v[0, h, at].astype(F32) + b_recv_v[1, h, at].astype(F32) for h in range(2)
        ]
        total = jnp.concatenate(halves, axis=1) + residual[at].astype(F32)
        rows = normalize(total, resid_gain[...]).astype(BF16)
        hidden[at] = rows
        total_v[at] = rows.astype(F32)
        return 0

    hear(5)
    lax.fori_loop(0, BLOCK // strip, norm_rows, 0, unroll=True)

    band_slots = 2 * PEERS * CAP

    def fill_slots(band):
        at = slice(band * band_slots, (band + 1) * band_slots)

        def one_tile(n, _):
            cols = pl.ds(pl.multiple_of(n * TILE, TILE), TILE)
            picked = jnp.dot(held[at, :], hidden[:, cols], preferred_element_type=F32)
            to = slice(band * 2 * PEERS, (band + 1) * 2 * PEERS)
            slots[to, :, cols] = picked.reshape(2 * PEERS, CAP, TILE).astype(BF16)
            return 0

        lax.fori_loop(0, width // TILE, one_tile, 0)

    for group in range(GROUPS):
        if group % 2 == 0:
            fill_slots(group // 2)
        if group == SELF_GROUP:
            pltpu.make_async_copy(slots.at[SELF], recv.at[SELF], d_recv.at[SELF]).start()
        for half in range(2):
            dz = step_along_z(group // 2, half)
            base = group * PEERS + half * SIDE

            def send(r, _, dz=dz, base=base, group=group):
                other = peer_at(z, y, core, dz, (1 - group % 2) * SIDE + r, 1)
                pltpu.make_async_remote_copy(
                    src_ref=slots.at[base + r], dst_ref=recv.at[base + r],
                    send_sem=d_send.at[base + r], recv_sem=d_recv.at[base + r],
                    device_id=(other, tp), device_id_type=MESH,
                ).start()
                return 0

            lax.fori_loop(1 if base == SELF else 0, SIDE, send, 0)

    def cross(c, src, dst, send_sem, recv_sem):
        return pltpu.make_async_remote_copy(
            src_ref=src.at[pl.ds(c * PEERS, PEERS)], dst_ref=dst.at[pl.ds(c * PEERS, PEERS)],
            send_sem=send_sem.at[c], recv_sem=recv_sem.at[c],
            device_id=(sp, row_partner), device_id_type=MESH,
        )

    def cross_back(c, half):
        at, cols = pl.ds(c * PEERS, PEERS), pl.ds(half * half_width, half_width)
        return pltpu.make_async_remote_copy(
            src_ref=xsend.at[at, :, cols], dst_ref=xret.at[at, :, cols],
            send_sem=b_send.at[2 * c + half], recv_sem=b_recv.at[2 * c + half],
            device_id=(sp, row_partner), device_id_type=MESH,
        )

    count = PEERS * CAP

    def arrive(group):
        def one(r, _):
            wait_for(recv.at[group * PEERS + r], d_recv.at[group * PEERS + r])
            return 0

        lax.fori_loop(0, PEERS, one, 0)
        cross(group, recv, xrecv, x_send, x_recv).start()

    def activations(c):
        cross(c, recv, xrecv, x_send, x_recv).wait_recv()
        at = pl.ds(c * PEERS, PEERS)
        rows_v[0:count] = recv[at].astype(F32).reshape(count, width).astype(BF16)
        rows_v[count : 2 * count] = xrecv[at].astype(F32).reshape(count, width).astype(BF16)

        def activate(j, _):
            half, col = j // 2, pl.multiple_of((j % 2) * TILE, TILE)
            g = jnp.dot(rows_v[...], gate_v[half, :, pl.ds(col, TILE)], preferred_element_type=F32)
            u = jnp.dot(rows_v[...], up_v[half, :, pl.ds(col, TILE)], preferred_element_type=F32)
            g = jnp.minimum(g, LIMIT)
            u = jnp.clip(u, -LIMIT, LIMIT)
            act = (u + 1.0) * g * jax.nn.sigmoid(SLOPE * g)
            act_v[c, :, pl.ds(pl.multiple_of(j * TILE, TILE), TILE)] = act.astype(BF16)
            return 0

        lax.fori_loop(0, 2 * half_units // TILE, activate, 0)

    def outputs(c, half):
        at = pl.ds(c * PEERS, PEERS)

        def project(n, _):
            cols = pl.ds(pl.multiple_of(half * half_width + n * TILE, TILE), TILE)
            result = jnp.dot(act_v[c], down_v[:, cols], preferred_element_type=F32)
            kept[c, :, cols] = result[0:count]
            xsend[at, :, cols] = result[count : 2 * count].reshape(PEERS, CAP, TILE).astype(BF16)
            return 0

        lax.fori_loop(0, half_width // TILE, project, 0)
        cross_back(c, half).start()

    def give_back(c, h):
        at, cols = pl.ds(c * PEERS, PEERS), pl.ds(pl.multiple_of(h * half_width, half_width), half_width)
        cross_back(c, h).wait_recv()
        total = kept[c, :, cols].reshape(PEERS, CAP, half_width) + xret[at, :, cols].astype(F32)
        fin[at, :, cols] = total.astype(BF16)
        for side in range(2):
            dz = step_along_z(c // 2, side)

            def send(r, _, dz=dz, side=side):
                k = c * PEERS + side * SIDE + r
                other = peer_at(z, y, core, dz, (1 - c % 2) * SIDE + r, -1)

                @pl.when(k != SELF)
                def away():
                    pltpu.make_async_remote_copy(
                        src_ref=fin.at[k, :, cols], dst_ref=ret.at[k, :, cols],
                        send_sem=r_send.at[2 * k + h], recv_sem=r_recv.at[2 * k + h],
                        device_id=(other, tp), device_id_type=MESH,
                    ).start()

                @pl.when(k == SELF)
                def here():
                    pltpu.make_async_copy(fin.at[k, :, cols], ret.at[k, :, cols], r_recv.at[2 * k + h]).start()

                return 0

            lax.fori_loop(0, SIDE, send, 0)

    def gather_band(band, _):
        def one(r, _):
            k = band * 2 * PEERS + r // 2
            wait_for(ret.at[k, :, pl.ds(0, half_width)], r_recv.at[2 * k + r % 2])
            return 0

        lax.fori_loop(0, 4 * PEERS, one, 0)
        own = share[:, pl.ds(pl.multiple_of(band * band_slots, band_slots), band_slots)]

        def one_tile(n, _):
            cols = pl.ds(pl.multiple_of(n * TILE, TILE), TILE)
            rows = ret[pl.ds(band * 2 * PEERS, 2 * PEERS), :, cols].astype(F32).reshape(band_slots, TILE).astype(BF16)
            both = jnp.dot(own, rows, preferred_element_type=F32)
            total_v[:, cols] += both[0:BLOCK] + both[BLOCK : 2 * BLOCK]
            return 0

        lax.fori_loop(0, width // TILE, one_tile, 0)
        return 0

    def unit_of(u):
        early = u < 2 * FIRST
        return jnp.where(early, u % FIRST, u // 2), jnp.where(early, u // FIRST, u % 2)

    arrive(0)
    for load in loads[1:]:
        load.wait()
    for s in swaps[:4]:
        s.wait_recv()
    arrive(1)

    def stage(u, _):
        c, h = unit_of(u)

        @pl.when((u == FIRST) | (u == 2 * FIRST))
        def waiting():
            give_back(*unit_of(u - FIRST // 2 - u // (2 * FIRST)))

        @pl.when(h == 0)
        def inner():
            activations(c)

        for half, first in ((0, 0), (1, FIRST)):

            @pl.when(u == first)
            def down_weights(half=half):
                swaps[4 + half].wait_recv()

        outputs(c, h)

        @pl.when((u >= FIRST) & (u < 2 * FIRST))
        def next_rows():
            arrive(u)

        @pl.when(u == 2 * FIRST - 1)
        def one_more():
            arrive(u + 1)

        @pl.when((u >= 2 * FIRST) & (h == 0) & (c < GROUPS - 3))
        def later_rows():
            arrive(c + 3)

        @pl.when((u == 1) | (u == 2 * FIRST))
        def soon():
            give_back(*unit_of(u - 1))

        @pl.when(u >= 2 * FIRST + 3)
        def later():
            give_back(*unit_of(u - 3))

        return 0

    lax.fori_loop(0, 2 * GROUPS, stage, 0)
    give_back(GROUPS - 2, 1)
    lax.fori_loop(0, 1, gather_band, 0)
    give_back(GROUPS - 1, 0)
    give_back(GROUPS - 1, 1)
    lax.fori_loop(1, BANDS - 1, gather_band, 0)
    for c in range(GROUPS):
        cross(c, recv, xrecv, x_send, x_recv).wait_send()
        for half in range(2):
            cross_back(c, half).wait_send()
    for copy in [halo_copy, *swaps, *stat_copies, *far_copies, *near_copies[0], *near_copies[1]]:
        copy.wait_send()

    def sent(k, _):
        @pl.when(k != SELF)
        def away():
            wait_for(recv.at[k], d_send.at[k])
            for h in range(2):
                wait_for(fin.at[k, :, pl.ds(0, half_width)], r_send.at[2 * k + h])

        return 0

    lax.fori_loop(0, N_SP, sent, 0)
    lax.fori_loop(BANDS - 1, BANDS, gather_band, 0)

    def last_norm(i, _):
        at = pl.ds(pl.multiple_of(i * strip, strip), strip)
        out[at] = normalize(total_v[at], out_gain[...]).astype(BF16)
        return 0

    lax.fori_loop(0, BLOCK // strip, last_norm, 0, unroll=True)


def shards(
    glu_value,
    glu_gate,
    conv_kernel,
    norm_gain,
    mix_weight,
    residual,
    resid_gain,
    expert_ids,
    route_weight,
    w_gate,
    w_up,
    w_down,
    out_gain,
):
    width = residual.shape[1]
    units = w_down.shape[1]
    channels = glu_value.shape[1]
    groups = channels // LANES
    experts = N_SP
    count = PEERS * CAP
    dma = pltpu.SemaphoreType.DMA
    vmem, hbm = pl.BlockSpec(memory_space=pltpu.VMEM), pl.BlockSpec(memory_space=pltpu.MemorySpace.HBM)
    moved = pltpu.VMEM((experts, CAP, width), BF16)
    return pl.pallas_call(
        layer_kernel,
        out_shape=jax.ShapeDtypeStruct((BLOCK, width), BF16),
        in_specs=[hbm] * 13,
        out_specs=vmem,
        scratch_shapes=[
            pltpu.VMEM(glu_value.shape, BF16),
            pltpu.VMEM(glu_gate.shape, BF16),
            pltpu.VMEM(conv_kernel.shape, F32),
            pltpu.VMEM((1, channels), F32),
            pltpu.VMEM(residual.shape, BF16),
            pltpu.VMEM((1, width), F32),
            pltpu.VMEM((1, width), F32),
            pltpu.VMEM((2, BLOCK), jnp.int32),
            pltpu.VMEM((2, BLOCK), F32),
            pltpu.VMEM((BLOCK, width), F32),
            pltpu.VMEM((groups, ROWS + HALO, LANES), F32),
            pltpu.VMEM((groups, HALO, LANES), BF16),
            pltpu.VMEM((groups, HALO, LANES), BF16),
            pltpu.VMEM((groups, ROWS, LANES), F32),
            pltpu.VMEM((ROWS, LANES), F32),
            pltpu.VMEM((LANES, ROWS), F32),
            pltpu.VMEM((8, ROWS), F32),
            pltpu.VMEM((N_TP - 1, 8, ROWS), F32),
            pltpu.VMEM((ROWS, channels), BF16),
            pltpu.VMEM((channels, width), BF16),
            pltpu.VMEM((2, BLOCK, width // 2), BF16),
            pltpu.VMEM((2, BLOCK, width // 2), BF16),
            pltpu.VMEM((2, 2, BLOCK, width // 2), BF16),
            pltpu.VMEM((2, 2, BLOCK, width // 2), BF16),
            pltpu.VMEM((2, BLOCK, width // 2), F32),
            pltpu.VMEM((BLOCK, width), BF16),
            pltpu.VMEM((experts * CAP, BLOCK), BF16),
            pltpu.VMEM((2 * BLOCK, experts * CAP), BF16),
            moved,
            moved,
            pltpu.VMEM((2, width, units), BF16),
            pltpu.VMEM((2, width, units), BF16),
            pltpu.VMEM((2 * units, width), BF16),
            moved,
            moved,
            pltpu.VMEM((2 * count, width), BF16),
            pltpu.VMEM((GROUPS, 2 * count, 2 * units), BF16),
            pltpu.VMEM((GROUPS, count, width), F32),
            moved,
            moved,
            moved,
            dma((experts,)), dma((experts,)),
            dma((GROUPS,)), dma((GROUPS,)),
            dma((2 * GROUPS,)), dma((2 * GROUPS,)),
            dma((2 * experts,)), dma((2 * experts,)),
            dma((6,)), dma((6,)), dma((13,)),
            pltpu.SemaphoreType.REGULAR((6,)),
            dma((2,)), dma((3,)), dma((3,)),
            dma((2,)), dma((2,)), dma((4,)), dma((4,)),
        ],
        compiler_params=pltpu.CompilerParams(
            collective_id=0, has_side_effects=True, vmem_limit_bytes=60 * 2**20
        ),
        name="layer",
    )(
        glu_value, glu_gate, conv_kernel, norm_gain[None], residual, resid_gain[None], out_gain[None],
        expert_ids.T, route_weight.T, mix_weight, w_gate, w_up, w_down,
    )


def solution(mesh):
    in_specs = (
        P("sp", "tp"),
        P("sp", "tp"),
        P(None, "tp"),
        P("tp"),
        P("tp", None),
        P(("sp", "tp"), None),
        P(),
        P(("sp", "tp"), None),
        P(("sp", "tp"), None),
        P("sp", None, "tp"),
        P("sp", None, "tp"),
        P("sp", "tp", None),
        P(),
    )
    out_specs = P(("sp", "tp"), None)
    return jax.shard_map(shards, mesh=mesh, in_specs=in_specs, out_specs=out_specs, check_vma=False)
```

```python
import jax
import jax.numpy as jnp
from jax import lax
from jax.experimental import pallas as pl
from jax.experimental.pallas import tpu as pltpu
from jax.sharding import PartitionSpec as P

DC = 2048
EPSILON = 1e-05
LIMIT = 7.0
SLOPE = 1.702
Z, Y, CORES, N_TP = 8, 4, 2, 4
PLANE = Y * CORES
N_SP = Z * PLANE
BANDS = 4
GROUPS = 2 * BANDS
FIRST = 2
SIDE = PLANE // 2
PEERS = 2 * SIDE
SELF_GROUP = 3
SELF = SELF_GROUP * PEERS + SIDE
CAP = 8
TILE = 256
LANES = 128
TAPS = 31
HALO = 32
ROWS = 512
BLOCK = 128
STRIPE = 64
MESH = pl.DeviceIdType.MESH
F32, BF16 = jnp.float32, jnp.bfloat16


def normalize(values, gain_vector):
    centre = jnp.mean(values, axis=-1, keepdims=True)
    spread = jnp.mean(jnp.square(values - centre), axis=-1, keepdims=True)
    return (values - centre) * lax.rsqrt(spread + EPSILON) * gain_vector


def position():
    sp, tp = lax.axis_index("sp"), lax.axis_index("tp")
    z, y, core = sp // PLANE, (sp // CORES) % Y, sp % CORES
    near, far = tp + 1 - 2 * (tp % 2), 3 - tp
    weight_partner = near * (1 - core) + far * core
    row_partner = near * core + far * (1 - core)
    return sp, tp, z, y, core, weight_partner, row_partner


def step_along_z(band, half):
    distance = 3 + band - 3 * (band // 2) - 2 * (band // 3)
    return distance if half == 0 else (Z - distance) * (1 - distance // 4)


def peer_at(z, y, core, dz, r, sign):
    return ((z + sign * dz + Z) % Z) * PLANE + ((y + sign * (r // 2) + Y) % Y) * CORES + (core + r % 2) % CORES


def wait_for(ref, sem):
    pltpu.make_async_copy(ref, ref, sem).wait()


def layer_kernel(
    value_h, gate_h, taps_h, norm_gain_h, residual_h, resid_gain_h, out_gain_h, ids_h, weights_h, mix_weight, w_gate, w_up, w_down,
    out,
    value, gate, taps, norm_gain, residual, resid_gain, out_gain, ids, weights, total_v, out_v, ext, halo_send, halo_recv, conv_v, stat_cols, stat_rows, stats_send, stats_recv, mix_in, mix_v,
    a_send_v, a_recv_v, b_send_v, b_recv_v, acc, hidden, held, share, slots, ret,
    gate_v, up_v, down_v, recv, xrecv, rows_v, act_v, kept, xsend, xret, fin,
    d_send, d_recv, x_send, x_recv, b_send, b_recv, r_send, r_recv, w_send, w_recv, l_sem,
    word, h_sem, s_send, s_recv, ra_send, ra_recv, rb_send, rb_recv,
):
    sp, tp, z, y, core, weight_partner, row_partner = position()
    barrier = pltpu.get_barrier_semaphore()

    along_z = [((z + d) % Z) * PLANE + sp % PLANE for d in (1, Z - 1)]
    along_y = [z * PLANE + ((y + d) % Y) * CORES + core for d in (1, Y - 1)]
    along_sp = [(sp + d) % N_SP for d in (1, N_SP - 1)]
    for other in along_sp + along_z + along_y:
        pl.semaphore_signal(barrier, inc=1, device_id=(other, tp), device_id_type=MESH)
    for i in range(1, N_TP):
        pl.semaphore_signal(barrier, inc=1, device_id=(sp, (tp + i) % N_TP), device_id_type=MESH)
    rounds = [along_z] * 3 + [along_y] * 2 + [[z * PLANE + y * CORES + 1 - core]]

    def tell(i):
        for other in rounds[i]:
            pl.semaphore_signal(word.at[i], inc=1, device_id=(other, tp), device_id_type=MESH)

    def hear(i):
        pl.semaphore_wait(word.at[i], len(rounds[i]))
        if i + 1 < len(rounds):
            tell(i + 1)

    width = w_down.shape[2]
    half_units = w_down.shape[1]
    half_width = width // 2
    channels = value.shape[1]
    first_loads = [
        pltpu.make_async_copy(src, dst, l_sem.at[4 + i])
        for i, (src, dst) in enumerate([
            (value_h, value), (gate_h, gate), (taps_h, taps), (norm_gain_h, norm_gain),
            (residual_h, residual), (resid_gain_h, resid_gain), (out_gain_h, out_gain), (ids_h, ids), (weights_h, weights),
        ])
    ]
    loads = [
        pltpu.make_async_copy(mix_weight, mix_v, l_sem.at[3]),
        pltpu.make_async_copy(w_gate.at[0], gate_v.at[0], l_sem.at[0]),
        pltpu.make_async_copy(w_up.at[0], up_v.at[0], l_sem.at[1]),
        pltpu.make_async_copy(w_down.at[0], down_v.at[0:half_units], l_sem.at[2]),
    ]
    for load in first_loads + loads:
        load.start()
    for load in first_loads[:2]:
        load.wait()

    lane_groups = channels // LANES

    def gated(rows, cols):
        product = value[rows, cols].astype(F32) * jax.nn.sigmoid(gate[rows, cols].astype(F32))
        return product.astype(BF16)

    for g in range(lane_groups):
        halo_send[g] = gated(pl.ds(ROWS - HALO, HALO), pl.ds(g * LANES, LANES))

    def gate_rows(i, _):
        for g in range(lane_groups):
            at = pl.ds(pl.multiple_of(i * STRIPE, STRIPE), STRIPE)
            to = pl.ds(pl.multiple_of(i * STRIPE + HALO, HALO), STRIPE)
            ext[g, to] = gated(at, pl.ds(g * LANES, LANES)).astype(F32)
        return 0

    lax.fori_loop(0, ROWS // STRIPE, gate_rows, 0)
    for load in first_loads[2:]:
        load.wait()
    pl.semaphore_wait(barrier, 6 + N_TP - 1)
    tell(0)
    halo_copy = pltpu.make_async_remote_copy(
        src_ref=halo_send, dst_ref=halo_recv, send_sem=h_sem.at[0], recv_sem=h_sem.at[1],
        device_id=(lax.rem(sp + 1, N_SP), tp), device_id_type=MESH,
    )
    halo_copy.start()

    def swap(i, src, dst):
        return pltpu.make_async_remote_copy(
            src_ref=src, dst_ref=dst, send_sem=w_send.at[i], recv_sem=w_recv.at[i],
            device_id=(sp, weight_partner), device_id_type=MESH,
        )

    def rows_of(ref, first, last):
        return ref.at[pl.ds(first, last - first)]

    cuts = (0, 768, 1536, 2048)
    swaps = [
        swap(i, w_gate.at[0, pl.ds(f, l - f)], gate_v.at[1, pl.ds(f, l - f)])
        for i, (f, l) in enumerate(zip(cuts, cuts[1:]))
    ] + [
        swap(3, w_up.at[0], up_v.at[1]),
    ] + [
        swap(
            4 + h, w_down.at[0, :, pl.ds(h * half_width, half_width)],
            down_v.at[pl.ds(half_units, half_units), pl.ds(h * half_width, half_width)],
        )
        for h in range(2)
    ]
    swaps[0].start()

    lane = lax.broadcasted_iota(jnp.int32, (STRIPE, LANES), 1)

    def convolve(i):
        first = pl.multiple_of(i * STRIPE, STRIPE)
        total, square = jnp.zeros((STRIPE, LANES), F32), jnp.zeros((STRIPE, LANES), F32)
        for g in range(lane_groups):
            sums = jnp.zeros((STRIPE, LANES), F32)
            for k in range(TAPS):
                tap = taps[k : k + 1, g * LANES : (g + 1) * LANES]
                sums = sums + tap * ext[g, pl.ds(first + (HALO - TAPS + 1 + k), STRIPE)]
            conv_v[g, pl.ds(first, STRIPE)] = sums
            total, square = total + sums, square + sums * sums
        total = jnp.sum(total, axis=1, keepdims=True)
        square = jnp.sum(square, axis=1, keepdims=True)
        stat_cols[pl.ds(first, STRIPE)] = jnp.where(lane == 0, total, jnp.where(lane == 1, square, 0.0))

    def convolve_step(i, _):
        convolve(i)
        return 0

    lax.fori_loop(1, ROWS // STRIPE, convolve_step, 0)
    hear(0)
    halo_copy.wait_recv()
    for g in range(lane_groups):
        ext[g, 0:HALO] = jnp.where(sp > 0, halo_recv[g].astype(F32), 0.0)
    convolve(0)
    for i in range(ROWS // LANES):
        at = slice(i * LANES, (i + 1) * LANES)
        stats_send[:, at] = jnp.transpose(stat_cols[at, :])[0:8]
    stat_copies = [
        pltpu.make_async_remote_copy(
            src_ref=stats_send, dst_ref=stats_recv.at[j - 1], send_sem=s_send.at[j - 1], recv_sem=s_recv.at[j - 1],
            device_id=(sp, (tp + j) % N_TP), device_id_type=MESH,
        )
        for j in (2, 1, 3)
    ]
    for c in stat_copies:
        c.start()
    swaps[1].start()

    hear(1)

    experts = N_SP
    spot = lax.broadcasted_iota(jnp.int32, (experts, BLOCK), 0)
    one = [(spot == ids[j : j + 1, :]).astype(BF16) for j in range(2)]
    before = lax.broadcasted_iota(jnp.int32, (BLOCK, BLOCK), 0) < lax.broadcasted_iota(jnp.int32, (BLOCK, BLOCK), 1)
    earlier = jnp.dot(one[0] + one[1], before.astype(BF16), preferred_element_type=F32)
    place = lax.broadcasted_iota(jnp.int32, (experts * CAP, experts), 0) // CAP
    group = place // PEERS
    band, r = group // 2, (1 - group % 2) * SIDE + place % SIDE
    step = jnp.where((place // SIDE) % 2 == 0, step_along_z(band, 0), step_along_z(band, 1))
    owner = peer_at(z, y, core, step, r, 1)
    spread_out = (owner == lax.broadcasted_iota(jnp.int32, (experts * CAP, experts), 1)).astype(BF16)
    rank = jnp.dot(spread_out, earlier.astype(BF16), preferred_element_type=F32)
    in_rank = rank == (lax.broadcasted_iota(jnp.int32, (experts * CAP, BLOCK), 0) % CAP).astype(F32)
    hits = [
        jnp.where(in_rank, jnp.dot(spread_out, o, preferred_element_type=F32), 0.0) for o in one
    ]
    held[...] = (hits[0] + hits[1]).astype(BF16)
    shares = hits[0] * weights[0:1, :] + hits[1] * weights[1:2, :]
    for i in range(experts * CAP // LANES):
        at = slice(i * LANES, (i + 1) * LANES)
        part = jnp.transpose(shares[at, :])
        high = part.astype(BF16)
        share[0:BLOCK, at] = high
        share[BLOCK : 2 * BLOCK, at] = (part - high.astype(F32)).astype(BF16)
    stat_rows[...] = jnp.zeros_like(stat_rows)
    hear(2)

    for c in stat_copies:
        c.wait_recv()
    sums = stats_send[...] + stats_recv[0] + stats_recv[1] + stats_recv[2]
    centre = sums[0:1] / DC
    scale = lax.rsqrt(sums[1:2] / DC - centre * centre + EPSILON)
    stat_rows[0:1] = centre
    stat_rows[1:2] = scale

    loads[0].wait()

    def mix_rows(b):
        at = pl.ds(pl.multiple_of(b * BLOCK, BLOCK), BLOCK)
        columns = jnp.transpose(stat_rows[:, at])
        for g in range(lane_groups):
            lanes = slice(g * LANES, (g + 1) * LANES)
            v = (conv_v[g, at] - columns[:, 0:1]) * columns[:, 1:2] * norm_gain[:, lanes]
            mix_in[at, lanes] = (v / (1.0 + jnp.exp(-v))).astype(BF16)

    def project_rows(b, half, into):
        at = pl.ds(pl.multiple_of(b * BLOCK, BLOCK), BLOCK)

        def one_tile(n, _):
            col = pl.multiple_of(n * TILE, TILE)
            cols = pl.ds(pl.multiple_of(half * half_width + n * TILE, TILE), TILE)
            into(pl.ds(col, TILE), jnp.dot(mix_in[at, :], mix_v[:, cols], preferred_element_type=F32))
            return 0

        lax.fori_loop(0, half_width // TILE, one_tile, 0)

    def to_neighbour(src, dst, send_sem, recv_sem, side):
        return pltpu.make_async_remote_copy(
            src_ref=src, dst_ref=dst, send_sem=send_sem, recv_sem=recv_sem,
            device_id=(sp, (tp + (1 if side == 0 else N_TP - 1)) % N_TP), device_id_type=MESH,
        )

    far_copies = [
        to_neighbour(a_send_v.at[i], a_recv_v.at[i], ra_send.at[i], ra_recv.at[i], i) for i in range(2)
    ]
    near_copies = [
        [
            to_neighbour(
                b_send_v.at[i, h], b_recv_v.at[i, h], rb_send.at[2 * i + h], rb_recv.at[2 * i + h], i
            )
            for h in range(2)
        ]
        for i in range(2)
    ]
    hear(3)
    far = (tp + 2) % N_TP
    sides = [(tp + 1) % N_TP, (tp + N_TP - 1) % N_TP]
    mix_rows(far)
    for i in range(2):

        def keep(cols, product, i=i):
            a_send_v[i, :, cols] = product.astype(BF16)

        project_rows(far, i, keep)
        far_copies[i].start()
    for i in range(2):
        mix_rows(sides[i])

        def keep(cols, product, i=i):
            b_send_v[i, 1 - i, :, cols] = product.astype(BF16)

        project_rows(sides[i], 1 - i, keep)
        near_copies[i][1 - i].start()
    for i in range(2):
        far_copies[i].wait_recv()

        def keep(cols, product, i=i):
            b_send_v[i, i, :, cols] = (product + a_recv_v[i, :, cols].astype(F32)).astype(BF16)

        project_rows(sides[i], i, keep)
        near_copies[i][i].start()
    for s in swaps[2:]:
        s.start()
    hear(4)
    mix_rows(tp)
    for h in range(2):

        def keep(cols, product, h=h):
            acc[h, :, cols] = product

        project_rows(tp, h, keep)
    for i in range(2):
        near_copies[i][1 - i].wait_recv()
    for i in range(2):
        near_copies[i][i].wait_recv()

    strip = 16

    def norm_rows(i, _):
        at = pl.ds(pl.multiple_of(i * strip, strip), strip)
        halves = [
            acc[h, at] + b_recv_v[0, h, at].astype(F32) + b_recv_v[1, h, at].astype(F32) for h in range(2)
        ]
        total = jnp.concatenate(halves, axis=1) + residual[at].astype(F32)
        rows = normalize(total, resid_gain[...]).astype(BF16)
        hidden[at] = rows
        total_v[at] = rows.astype(F32)
        return 0

    hear(5)
    lax.fori_loop(0, BLOCK // strip, norm_rows, 0, unroll=True)

    band_slots = 2 * PEERS * CAP

    def fill_slots(band):
        at = slice(band * band_slots, (band + 1) * band_slots)

        def one_tile(n, _):
            cols = pl.ds(pl.multiple_of(n * TILE, TILE), TILE)
            picked = jnp.dot(held[at, :], hidden[:, cols], preferred_element_type=F32)
            to = slice(band * 2 * PEERS, (band + 1) * 2 * PEERS)
            slots[to, :, cols] = picked.reshape(2 * PEERS, CAP, TILE).astype(BF16)
            return 0

        lax.fori_loop(0, width // TILE, one_tile, 0)

    for group in range(GROUPS):
        if group % 2 == 0:
            fill_slots(group // 2)
        if group == SELF_GROUP:
            pltpu.make_async_copy(slots.at[SELF], recv.at[SELF], d_recv.at[SELF_GROUP]).start()
        for half in range(2):
            dz = step_along_z(group // 2, half)
            base = group * PEERS + half * SIDE

            def send(r, _, dz=dz, base=base, group=group):
                other = peer_at(z, y, core, dz, (1 - group % 2) * SIDE + r, 1)
                pltpu.make_async_remote_copy(
                    src_ref=slots.at[base + r], dst_ref=recv.at[base + r],
                    send_sem=d_send.at[0], recv_sem=d_recv.at[group],
                    device_id=(other, tp), device_id_type=MESH,
                ).start()
                return 0

            lax.fori_loop(1 if base == SELF else 0, SIDE, send, 0)

    def cross(c, src, dst, send_sem, recv_sem):
        return pltpu.make_async_remote_copy(
            src_ref=src.at[pl.ds(c * PEERS, PEERS)], dst_ref=dst.at[pl.ds(c * PEERS, PEERS)],
            send_sem=send_sem.at[0], recv_sem=recv_sem.at[c],
            device_id=(sp, row_partner), device_id_type=MESH,
        )

    def cross_back(c, half):
        at, cols = pl.ds(c * PEERS, PEERS), pl.ds(half * half_width, half_width)
        return pltpu.make_async_remote_copy(
            src_ref=xsend.at[at, :, cols], dst_ref=xret.at[at, :, cols],
            send_sem=b_send.at[0], recv_sem=b_recv.at[2 * c + half],
            device_id=(sp, row_partner), device_id_type=MESH,
        )

    count = PEERS * CAP

    def arrive(group):
        wait_for(recv.at[pl.ds(group * PEERS, PEERS)], d_recv.at[group])
        cross(group, recv, xrecv, x_send, x_recv).start()

    def activations(c):
        cross(c, recv, xrecv, x_send, x_recv).wait_recv()
        at = pl.ds(c * PEERS, PEERS)
        rows_v[0:count] = recv[at].astype(F32).reshape(count, width).astype(BF16)
        rows_v[count : 2 * count] = xrecv[at].astype(F32).reshape(count, width).astype(BF16)

        def activate(j, _):
            half, col = j // 2, pl.multiple_of((j % 2) * TILE, TILE)
            g = jnp.dot(rows_v[...], gate_v[half, :, pl.ds(col, TILE)], preferred_element_type=F32)
            u = jnp.dot(rows_v[...], up_v[half, :, pl.ds(col, TILE)], preferred_element_type=F32)
            g = jnp.minimum(g, LIMIT)
            u = jnp.clip(u, -LIMIT, LIMIT)
            act = (u + 1.0) * g * jax.nn.sigmoid(SLOPE * g)
            act_v[c, :, pl.ds(pl.multiple_of(j * TILE, TILE), TILE)] = act.astype(BF16)
            return 0

        lax.fori_loop(0, 2 * half_units // TILE, activate, 0)

    def outputs(c, half):
        at = pl.ds(c * PEERS, PEERS)

        def project(n, _):
            cols = pl.ds(pl.multiple_of(half * half_width + n * TILE, TILE), TILE)
            result = jnp.dot(act_v[c], down_v[:, cols], preferred_element_type=F32)
            kept[c, :, cols] = result[0:count]
            xsend[at, :, cols] = result[count : 2 * count].reshape(PEERS, CAP, TILE).astype(BF16)
            return 0

        lax.fori_loop(0, half_width // TILE, project, 0)
        cross_back(c, half).start()

    def give_back(c, h):
        at, cols = pl.ds(c * PEERS, PEERS), pl.ds(pl.multiple_of(h * half_width, half_width), half_width)
        cross_back(c, h).wait_recv()
        total = kept[c, :, cols].reshape(PEERS, CAP, half_width) + xret[at, :, cols].astype(F32)
        fin[at, :, cols] = total.astype(BF16)
        for side in range(2):
            dz = step_along_z(c // 2, side)

            def send(r, _, dz=dz, side=side):
                k = c * PEERS + side * SIDE + r
                other = peer_at(z, y, core, dz, (1 - c % 2) * SIDE + r, -1)

                @pl.when(k != SELF)
                def away():
                    pltpu.make_async_remote_copy(
                        src_ref=fin.at[k, :, cols], dst_ref=ret.at[k, :, cols],
                        send_sem=r_send.at[0], recv_sem=r_recv.at[2 * c + h],
                        device_id=(other, tp), device_id_type=MESH,
                    ).start()

                @pl.when(k == SELF)
                def here():
                    pltpu.make_async_copy(fin.at[k, :, cols], ret.at[k, :, cols], r_recv.at[2 * c + h]).start()

                return 0

            lax.fori_loop(0, SIDE, send, 0)

    def gather_band(band, _):
        for i in range(2):
            group = 2 * band + i
            for h in range(2):
                rows = ret.at[pl.ds(group * PEERS, PEERS), :, pl.ds(h * half_width, half_width)]
                wait_for(rows, r_recv.at[2 * group + h])

        own = share[:, pl.ds(pl.multiple_of(band * band_slots, band_slots), band_slots)]

        def one_tile(n, _):
            cols = pl.ds(pl.multiple_of(n * TILE, TILE), TILE)
            rows = ret[pl.ds(band * 2 * PEERS, 2 * PEERS), :, cols].astype(F32).reshape(band_slots, TILE).astype(BF16)
            both = jnp.dot(own, rows, preferred_element_type=F32)
            total_v[:, cols] += both[0:BLOCK] + both[BLOCK : 2 * BLOCK]
            return 0

        lax.fori_loop(0, width // TILE, one_tile, 0)
        return 0

    def unit_of(u):
        early = u < 2 * FIRST
        return jnp.where(early, u % FIRST, u // 2), jnp.where(early, u // FIRST, u % 2)

    arrive(0)
    for load in loads[1:]:
        load.wait()
    for s in swaps[:4]:
        s.wait_recv()
    arrive(1)

    def stage(u, _):
        c, h = unit_of(u)

        @pl.when(u == FIRST)
        def waiting():
            give_back(1, 0)

        @pl.when(u == 2 * FIRST)
        def both():
            give_back(0, 1)
            give_back(1, 1)

        @pl.when(h == 0)
        def inner():
            activations(c)

        for half, first in ((0, 0), (1, FIRST)):

            @pl.when(u == first)
            def down_weights(half=half):
                swaps[4 + half].wait_recv()

        outputs(c, h)

        @pl.when(u == 2 * FIRST - 1)
        def next_rows():
            for group in range(FIRST, FIRST + 3):
                arrive(group)

        @pl.when((u >= 2 * FIRST) & (h == 0) & (c < GROUPS - 3))
        def later_rows():
            arrive(c + 3)

        @pl.when(u == 1)
        def soon():
            give_back(0, 0)

        @pl.when(u >= 2 * FIRST + 3)
        def later():
            give_back(*unit_of(u - 3))

        return 0

    lax.fori_loop(0, 2 * GROUPS, stage, 0)
    give_back(GROUPS - 2, 1)
    lax.fori_loop(0, 1, gather_band, 0)
    give_back(GROUPS - 1, 0)
    give_back(GROUPS - 1, 1)
    lax.fori_loop(1, BANDS - 1, gather_band, 0)
    wait_for(recv, x_send.at[0])
    wait_for(xsend, b_send.at[0])
    for copy in [halo_copy, *swaps, *stat_copies, *far_copies, *near_copies[0], *near_copies[1]]:
        copy.wait_send()

    wait_for(recv.at[pl.ds(0, N_SP - 1)], d_send.at[0])
    wait_for(fin.at[pl.ds(0, N_SP - 1)], r_send.at[0])
    lax.fori_loop(BANDS - 1, BANDS, gather_band, 0)

    def last_norm(i, _):
        at = pl.ds(pl.multiple_of(i * strip, strip), strip)
        out_v[at] = normalize(total_v[at], out_gain[...]).astype(BF16)
        return 0

    pieces = []
    for i in range(2):
        at = pl.ds(i * BLOCK // 2, BLOCK // 2)
        lax.fori_loop(i * BLOCK // strip // 2, (i + 1) * BLOCK // strip // 2, last_norm, 0, unroll=True)
        pieces.append(pltpu.make_async_copy(out_v.at[at], out.at[at], l_sem.at[i]))
        pieces[-1].start()
    for piece in pieces:
        piece.wait()


def shards(
    glu_value,
    glu_gate,
    conv_kernel,
    norm_gain,
    mix_weight,
    residual,
    resid_gain,
    expert_ids,
    route_weight,
    w_gate,
    w_up,
    w_down,
    out_gain,
):
    width = residual.shape[1]
    units = w_down.shape[1]
    channels = glu_value.shape[1]
    groups = channels // LANES
    experts = N_SP
    count = PEERS * CAP
    dma = pltpu.SemaphoreType.DMA
    vmem, hbm = pl.BlockSpec(memory_space=pltpu.VMEM), pl.BlockSpec(memory_space=pltpu.MemorySpace.HBM)
    moved = pltpu.VMEM((experts, CAP, width), BF16)
    return pl.pallas_call(
        layer_kernel,
        out_shape=jax.ShapeDtypeStruct((BLOCK, width), BF16),
        in_specs=[hbm] * 13,
        out_specs=hbm,
        scratch_shapes=[
            pltpu.VMEM(glu_value.shape, BF16),
            pltpu.VMEM(glu_gate.shape, BF16),
            pltpu.VMEM(conv_kernel.shape, F32),
            pltpu.VMEM((1, channels), F32),
            pltpu.VMEM(residual.shape, BF16),
            pltpu.VMEM((1, width), F32),
            pltpu.VMEM((1, width), F32),
            pltpu.VMEM((2, BLOCK), jnp.int32),
            pltpu.VMEM((2, BLOCK), F32),
            pltpu.VMEM((BLOCK, width), F32),
            pltpu.VMEM((BLOCK, width), BF16),
            pltpu.VMEM((groups, ROWS + HALO, LANES), F32),
            pltpu.VMEM((groups, HALO, LANES), BF16),
            pltpu.VMEM((groups, HALO, LANES), BF16),
            pltpu.VMEM((groups, ROWS, LANES), F32),
            pltpu.VMEM((ROWS, LANES), F32),
            pltpu.VMEM((LANES, ROWS), F32),
            pltpu.VMEM((8, ROWS), F32),
            pltpu.VMEM((N_TP - 1, 8, ROWS), F32),
            pltpu.VMEM((ROWS, channels), BF16),
            pltpu.VMEM((channels, width), BF16),
            pltpu.VMEM((2, BLOCK, width // 2), BF16),
            pltpu.VMEM((2, BLOCK, width // 2), BF16),
            pltpu.VMEM((2, 2, BLOCK, width // 2), BF16),
            pltpu.VMEM((2, 2, BLOCK, width // 2), BF16),
            pltpu.VMEM((2, BLOCK, width // 2), F32),
            pltpu.VMEM((BLOCK, width), BF16),
            pltpu.VMEM((experts * CAP, BLOCK), BF16),
            pltpu.VMEM((2 * BLOCK, experts * CAP), BF16),
            moved,
            moved,
            pltpu.VMEM((2, width, units), BF16),
            pltpu.VMEM((2, width, units), BF16),
            pltpu.VMEM((2 * units, width), BF16),
            moved,
            moved,
            pltpu.VMEM((2 * count, width), BF16),
            pltpu.VMEM((GROUPS, 2 * count, 2 * units), BF16),
            pltpu.VMEM((GROUPS, count, width), F32),
            moved,
            moved,
            moved,
            dma((1,)), dma((GROUPS,)),
            dma((1,)), dma((GROUPS,)),
            dma((1,)), dma((2 * GROUPS,)),
            dma((1,)), dma((2 * GROUPS,)),
            dma((6,)), dma((6,)), dma((13,)),
            pltpu.SemaphoreType.REGULAR((6,)),
            dma((2,)), dma((3,)), dma((3,)),
            dma((2,)), dma((2,)), dma((4,)), dma((4,)),
        ],
        compiler_params=pltpu.CompilerParams(
            collective_id=0, has_side_effects=True, vmem_limit_bytes=60 * 2**20
        ),
        name="layer",
    )(
        glu_value, glu_gate, conv_kernel, norm_gain[None], residual, resid_gain[None], out_gain[None],
        expert_ids.T, route_weight.T, mix_weight, w_gate, w_up, w_down,
    )


def solution(mesh):
    in_specs = (
        P("sp", "tp"),
        P("sp", "tp"),
        P(None, "tp"),
        P("tp"),
        P("tp", None),
        P(("sp", "tp"), None),
        P(),
        P(("sp", "tp"), None),
        P(("sp", "tp"), None),
        P("sp", None, "tp"),
        P("sp", None, "tp"),
        P("sp", "tp", None),
        P(),
    )
    out_specs = P(("sp", "tp"), None)
    return jax.shard_map(shards, mesh=mesh, in_specs=in_specs, out_specs=out_specs, check_vma=False)
```
